32 devices in a mesh: sp: 16 (over z, y, x), tp: 2 (over core).
Axes of the slice: x: 2, y: 2, z: 4, core: 2. Of those that a mesh axis runs over, the one named last changes fastest.
Arguments:
- query: bfloat16 [2048, 2048], P('sp', 'tp'), may hold values from -6 to 6
- forget_logit: bfloat16 [2048, 2048], P('sp', 'tp'), may hold values from -7.5 to 7.5
- value: bfloat16 [2048, 2048], P('sp', 'tp'), may hold values from -6 to 6
- out_gate: bfloat16 [2048, 2048], P('sp', 'tp'), may hold values from -6 to 6
- lower_bound: float32 [2048], P('tp'), may hold values from 0.9 to 1, as said below
- head_gain: float32 [2048], P('tp'), may hold values from 0.1 to 1.9
- residual_in: bfloat16 [2048, 2048], P(('sp', 'tp')), may hold values from -6 to 6
- w_out: bfloat16 [2048, 2048], replicated, may hold values from -0.125 to 0.125
- ffn_gain: float32 [2048], replicated, may hold values from 0.1 to 1.9
- routing: int32 [2048, 2], P(('sp', 'tp')), may hold values from 0 to 15, all different within a row; in each aligned block of 64 rows (0 to 63, 64 to 127, ...) at most 16 rows name the same one
- route_weight: float32 [2048, 2], P(('sp', 'tp')), may hold values from 0.25 to 1
- expert_gate: bfloat16 [16, 2048, 1024], P('sp', None, 'tp'), may hold values from -0.125 to 0.125
- expert_up: bfloat16 [16, 2048, 1024], P('sp', None, 'tp'), may hold values from -0.125 to 0.125
- expert_down: bfloat16 [16, 1024, 2048], P('sp', 'tp'), may hold values from -0.1875 to 0.1875
Outputs:
- layer_out: bfloat16 [2048, 2048], P(('sp', 'tp'))
The draws below stay inside these ranges and needn't reach their ends.
Inputs may be any that keep to these rules, and one draw needn't show every extreme that they name: `routing`: each row names 2 different experts. In each aligned block of 64 rows (the rows of one device) no expert is named by more than 16 rows, a bound that some blocks reach. 1 - lower_bound is at least 1 / 4096.
All inputs are finite; a program needn't handle non-finite values.
Results may differ from the reference program's by a relative error of at most 0.012.
Values may be sent and summed in bfloat16 or wider, within the bound.
A program may use at most 128 MiB of HBM per device.

```python
import math
import jax
import jax.numpy as jnp
import numpy as np
from jax import lax

D = 2048
HEADS = 16
HEAD_DIM = 128
FF = 1024
TOP_K = 2
BLOCK = 16
TOKENS = 2048
HALF = 64
EXPERTS = 16
CAP = 16
N_SP = 16
N_TP = 2


def draw_lower_bound(key, part):
    order_key, slow_key, fast_key, middle_key = jax.random.split(jax.random.fold_in(key, 11), 4)
    slow_count = HEADS // 2
    middle_count = max(1, HEADS // 5)
    ranks = jax.random.permutation(order_key, HEADS)
    middle_heads = ranks < middle_count
    slow_heads = ranks < slow_count
    slow_gap = jnp.exp(jax.random.uniform(slow_key, (HEADS, HEAD_DIM), jnp.float32, jnp.log(0.5), jnp.log(3.0))) / TOKENS
    fast_gap = jnp.exp(jax.random.uniform(fast_key, (HEADS, HEAD_DIM), jnp.float32, jnp.log(0.03), jnp.log(0.1)))
    middle_gap = jnp.exp(jax.random.uniform(middle_key, (HEADS, HEAD_DIM), jnp.float32, jnp.log(0.002), jnp.log(0.008)))
    gap_values = jnp.where(slow_heads[:, None], slow_gap, fast_gap)
    gap_values = jnp.where(middle_heads[:, None], middle_gap, gap_values)
    return (1.0 - gap_values).reshape(-1).astype(jnp.float32)


def draw_forget_logit(key, part):
    rough_key, span_key, wide_key = jax.random.split(jax.random.fold_in(key, 23), 3)
    width = HEADS * HEAD_DIM
    rows = jnp.arange(TOKENS)
    rough = jax.random.normal(rough_key, (TOKENS, width), jnp.float32)
    offsets = jax.random.uniform(span_key, (TOKENS // 128 + 1, width), jnp.float32, -1.5, 1.5)
    wide = jax.random.uniform(wide_key, (TOKENS // 1024 + 1, HEADS), jnp.float32, -1.5, 6.0)
    wide_full = jnp.repeat(wide, HEAD_DIM, axis=1)
    values = rough + offsets[rows // 128] + wide_full[rows // 1024]
    return jnp.clip(values, -7.5, 7.5).astype(jnp.bfloat16)


def block_scale(rng, extent, shards, low, top_value):
    loudness = 1.0
    for dim, parts in shards:
        steps = jax.random.uniform(jax.random.fold_in(jax.random.fold_in(rng, 6), dim), (parts,), jnp.float32, low / len(shards), top_value / len(shards))
        loudness = loudness * jnp.repeat(jnp.exp(steps), extent[dim] // parts).reshape((-1,) + (1,) * (len(extent) - 1 - dim))
    return loudness


def routed_block(key, own, number, rows, number_of, top, most, skew):
    order = jax.random.permutation(key, number_of)
    heavy_load, usual = load_shares(number_of, rows * top, most, skew, True), load_shares(number_of, rows * top, most, skew, False)
    places = jnp.arange(number_of)

    def named(sizes, rotation):
        used = int((sizes > 0).sum())
        fixed = max(1, used // 4)
        shifted = fixed + (places - fixed + rotation * (used - fixed)) % max(1, number_of - fixed)
        return jnp.zeros((number_of,), jnp.int32).at[order[jnp.where(places < fixed, places, shifted)]].set(jnp.asarray(sizes, jnp.int32))

    sizes = jnp.where(number % 4 == 0, named(heavy_load, number // 4), named(usual, number - number // 4 - 1))
    mixed = jax.random.permutation(jax.random.fold_in(own, 3), number_of)
    donor, taker = mixed[0:number_of // 2 * 2:2], mixed[1:number_of // 2 * 2:2]
    room = jnp.minimum(sizes[donor] - 1, most - sizes[taker]) // 2
    room = jnp.where((donor == order[0]) | (taker == order[0]) | (sizes[taker] == 0), 0, jnp.maximum(room, 0))
    shifted = jax.random.randint(jax.random.fold_in(own, 4), (number_of // 2,), 0, 1 << 20) % (room + 1)
    sizes = sizes.at[donor].add(-shifted).at[taker].add(shifted)
    labels = jnp.searchsorted(jnp.cumsum(sizes), jnp.arange(rows * top), side="right").astype(jnp.int32)
    table = labels.reshape(top, rows).T
    table = table[jax.random.permutation(jax.random.fold_in(own, 1), rows)]
    rotation = jax.random.randint(jax.random.fold_in(own, 2), (rows, 1), 0, top)
    return jnp.take_along_axis(table, (jnp.arange(top)[None, :] + rotation) % top, axis=1)


def load_shares(count, total, bound, slope, full):
    weights = [(1 << 20) // math.isqrt(rank ** slope) + 1 for rank in range(1, count + 1)]
    largest = bound if full else min(bound, max(-(-total // count), total * weights[0] // sum(weights)))
    least = 1 if total - largest >= count - 1 else 0
    holding, surplus = [largest] + [least] * (count - 1), total - largest - least * (count - 1)
    while surplus > 0:
        free = [i for i in range(1, count) if holding[i] < largest] or [i for i in range(1, count) if holding[i] < bound]
        pool, left = sum([weights[i] for i in free]), surplus
        for i in free:
            more = min(bound - holding[i], max(1, left * weights[i] // pool), surplus)
            holding[i] = holding[i] + more
            surplus = surplus - more
    return np.array(holding)


def scatter_about(stream_key, shape, deviation, bound, cuts=(), kind=jnp.bfloat16):
    values = deviation * jax.random.normal(stream_key, shape, jnp.float32)
    if cuts:
        values = values * block_scale(stream_key, shape, cuts, -0.22, 0.18)
    return jnp.clip(values, -bound, bound).astype(kind)


def setup_inputs(seed: int = 0) -> dict:
    arg_keys = jax.random.split(jax.random.key(seed), 15)
    query = scatter_about(arg_keys[0], (TOKENS, HEADS * HEAD_DIM), 1.0, 6.0, ((0, 16), (1, 2)))
    forget_logit = draw_forget_logit(jax.random.fold_in(arg_keys[14], 71), 0)
    value = scatter_about(arg_keys[2], (TOKENS, HEADS * HEAD_DIM), 1.0, 6.0, ((0, 16), (1, 2)))
    out_gate = scatter_about(arg_keys[3], (TOKENS, HEADS * HEAD_DIM), 1.0, 6.0, ((0, 16), (1, 2)))
    lower_bound = draw_lower_bound(jax.random.fold_in(arg_keys[14], 71), 0)
    head_gain = jnp.clip(1.0 + 0.18 * jax.random.normal(arg_keys[5], (HEADS * HEAD_DIM,), jnp.float32), 0.1, 1.9)
    residual_in = scatter_about(arg_keys[6], (TOKENS, D), 1.0, 6.0, ((0, 32),))
    w_out = scatter_about(arg_keys[7], (HEADS * HEAD_DIM, D), (HEADS * HEAD_DIM) ** -0.5, 0.125)
    ffn_gain = jnp.clip(1.0 + 0.18 * jax.random.normal(arg_keys[8], (D,), jnp.float32), 0.1, 1.9)
    routing_keys = jax.random.split(jax.random.fold_in(arg_keys[9], 1), TOKENS // HALF)
    routing_turns = jax.random.permutation(jax.random.fold_in(arg_keys[9], 3), TOKENS // HALF)
    routing = jax.vmap(lambda own, number: routed_block(jax.random.fold_in(arg_keys[9], 2), own, number, HALF, EXPERTS, TOP_K, CAP, 2))(routing_keys, routing_turns).reshape((TOKENS, TOP_K))
    route_weight = jnp.clip(0.25 + 0.75 * jax.random.uniform(arg_keys[10], (TOKENS, TOP_K), jnp.float32) ** block_scale(arg_keys[10], (TOKENS, TOP_K), ((0, 32),), -0.2, 0.2), 0.25, 1.0)
    expert_gate = scatter_about(arg_keys[11], (EXPERTS, D, FF), D ** -0.5, 0.125, ((0, 16), (2, 2)))
    expert_up = scatter_about(arg_keys[12], (EXPERTS, D, FF), D ** -0.5, 0.125, ((0, 16), (2, 2)))
    expert_down = scatter_about(arg_keys[13], (EXPERTS, FF, D), FF ** -0.5, 0.1875, ((0, 16), (1, 2)))
    return {"query": query, "forget_logit": forget_logit, "value": value, "out_gate": out_gate, "lower_bound": lower_bound, "head_gain": head_gain, "residual_in": residual_in, "w_out": w_out, "ffn_gain": ffn_gain, "routing": routing, "route_weight": route_weight, "expert_gate": expert_gate, "expert_up": expert_up, "expert_down": expert_down}


epsilon = 1e-06
highest = lax.Precision.HIGHEST

def recurrence(queries, log_forget, key_gate, values):
    blocks = queries.shape[0] // BLOCK

    def to_blocks(table):
        return table.reshape(blocks, BLOCK, HEADS, HEAD_DIM)
    causal = jnp.arange(BLOCK)[:, None] >= jnp.arange(BLOCK)[None, :]

    def advance(state, inputs):
        query_b, forget_b, key_b, value_b = inputs
        cumulative = jnp.cumsum(forget_b, axis=0)
        log_gaps = cumulative[:, None] - cumulative[None, :]
        decays = jnp.exp(jnp.where(causal[:, :, None, None], log_gaps, -jnp.inf))
        scores = jnp.einsum('thd,shd,tshd->hts', query_b, key_b, decays, precision=highest)
        result = jnp.einsum('hts,shv->thv', scores, value_b, precision=highest)
        result = result + jnp.einsum('thd,hdv->thv', query_b * jnp.exp(cumulative), state, precision=highest)
        last_log = cumulative[-1]
        weighted = key_b * jnp.exp(last_log[None] - cumulative)
        state = jnp.exp(last_log)[:, :, None] * state + jnp.einsum('shd,shv->hdv', weighted, value_b, precision=highest)
        return (state, result)
    initial = jnp.zeros((HEADS, HEAD_DIM, HEAD_DIM), jnp.float32)
    _, head_out = lax.scan(advance, initial, (to_blocks(queries), to_blocks(log_forget), to_blocks(key_gate), to_blocks(values)))
    return head_out.reshape(-1, HEADS, HEAD_DIM)

def expert_pass(normed, routing, route_weight, expert_gate, expert_up, expert_down):
    flat_routes = routing.reshape(-1)
    flat_weights = route_weight.reshape(-1)
    most_rows = N_SP * N_TP * CAP

    def visit(running, inputs):
        expert_id, gate_w, up_w, down_w = inputs
        matches = flat_routes == expert_id
        slots_found = jnp.nonzero(matches, size=most_rows, fill_value=0)[0]
        filled = jnp.arange(most_rows) < jnp.sum(matches)
        owners = slots_found // TOP_K
        taken = normed[owners]
        gate_part = jnp.dot(taken, gate_w, preferred_element_type=jnp.float32)
        up_part = jnp.dot(taken, up_w, preferred_element_type=jnp.float32)
        hidden = (jax.nn.silu(gate_part) * up_part).astype(jnp.bfloat16)
        expert_out = jnp.dot(hidden, down_w, preferred_element_type=jnp.float32).astype(jnp.bfloat16)
        scaled = jnp.where(filled, flat_weights[slots_found], 0.0)
        running = running.at[owners].add(expert_out.astype(jnp.float32) * scaled[:, None])
        return (running, None)
    initial = jnp.zeros(normed.shape, jnp.float32)
    expert_ids = jnp.arange(EXPERTS, dtype=jnp.int32)
    summed, _ = lax.scan(visit, initial, (expert_ids, expert_gate, expert_up, expert_down))
    return summed

def reference(query, forget_logit, value, out_gate, lower_bound, head_gain, residual_in, w_out, ffn_gain, routing, route_weight, expert_gate, expert_up, expert_down):
    positions = query.shape[0]
    grid = (positions, HEADS, HEAD_DIM)
    floor_gate = lower_bound.reshape(HEADS, HEAD_DIM)
    logits = forget_logit.astype(jnp.float32).reshape(grid)
    log_forget = jnp.logaddexp(jnp.log(floor_gate), jnp.log1p(-floor_gate) + jax.nn.log_sigmoid(logits))
    key_gate = (1.0 - floor_gate) * jax.nn.sigmoid(-logits)
    head_out = recurrence(query.astype(jnp.float32).reshape(grid), log_forget, key_gate, value.astype(jnp.float32).reshape(grid))
    normed_heads = head_out * lax.rsqrt(lax.optimization_barrier(jnp.mean(head_out * head_out, axis=-1, keepdims=True)) + epsilon)
    gates = jax.nn.silu(out_gate.astype(jnp.float32).reshape(grid))
    mixed = (normed_heads * head_gain.reshape(HEADS, HEAD_DIM) * gates).astype(jnp.bfloat16).reshape(positions, -1)
    projected = jnp.dot(mixed, w_out, preferred_element_type=jnp.float32)
    updated = (residual_in.astype(jnp.float32) + projected).astype(jnp.bfloat16)
    updated_f = updated.astype(jnp.float32)
    normed = (updated_f * lax.rsqrt(lax.optimization_barrier(jnp.mean(updated_f * updated_f, axis=-1, keepdims=True)) + epsilon) * ffn_gain).astype(jnp.bfloat16)
    expert_sum = expert_pass(normed, routing, route_weight, expert_gate, expert_up, expert_down)
    return (updated_f + expert_sum).astype(jnp.bfloat16)
```

```python
import functools

import jax
import jax.numpy as jnp
from jax import lax
from jax.experimental import pallas as pl
from jax.experimental.pallas import tpu as pltpu
from jax.sharding import PartitionSpec as P

HEAD_DIM = 128
MESH = pl.DeviceIdType.MESH
epsilon = 1e-06
f32 = jnp.float32
bf16 = jnp.bfloat16
NT = (((1,), (1,)), ((), ()))
TN = (((0,), (0,)), ((), ()))


def dot(a, b, dims=(((1,), (0,)), ((), ())), precision=None):
    return lax.dot_general(a, b, dims, precision=precision, preferred_element_type=f32)


def rows_of(index, count):
    return pl.ds(pl.multiple_of(index * count, count), count)


def greet(n):
    me, core = lax.axis_index("sp"), lax.axis_index("tp")
    barrier = pltpu.get_barrier_semaphore()
    pl.semaphore_signal(barrier, inc=1, device_id={"tp": 1 - core}, device_id_type=MESH)

    @pl.loop(1, n)
    def _(r):
        pl.semaphore_signal(
            barrier, inc=1, device_id={"sp": lax.rem(me + r, n)}, device_id_type=MESH
        )

    return barrier


def partner(me, r):
    other = me
    step = 1
    while step <= r:
        if r & step:
            other = other + step * (1 - 2 * (me // step % 2))
        step *= 2
    return other


def layer_kernel(
    n, cap,
    query_h, logit_h, value_h, gate_h, bound_h, gain_h, residual_h, ffn_gain_h, routing_h,
    weight_h, w_hbm, g_hbm, u_hbm, d_hbm,
    layer_out,
    query, logit, value, gate, bound, gain, residual, ffn_gain, routing, weight,
    w_out, q_scr, k_scr, ho, st_send, st_recv, dec_send, dec_recv, ret_send, ret_recv,
    mixed, regrouped, proj,
    wg, wu, wd, gated, normed, pick, comb, info_send, info_recv,
    outbox, arrived, hidden, result, returned, dense_in, relay_out, relay_in, dense_out, dense_ret,
    in_sem, w_sem, s_sem, r_sem, ds_sem, dr_sem, bs_sem, br_sem, ms_sem, mr_sem,
    l_sem, ps_sem, pr_sem, is_sem, ir_sem, xs_sem, xr_sem, ys_sem, yr_sem,
    vs_sem, vr_sem, fs_sem, fr_sem, gs_sem, gr_sem, es_sem, er_sem,
):
    me, core = lax.axis_index("sp"), lax.axis_index("tp")
    length, width = query.shape
    heads = width // HEAD_DIM
    groups, piece = st_recv.shape[0], st_recv.shape[2]
    per = heads // groups
    half = length // 2
    moves = [
        pltpu.make_async_copy(src, dst, in_sem.at[i])
        for i, (src, dst) in enumerate((
            (logit_h, logit), (bound_h, bound), (query_h, query), (value_h, value),
            (routing_h, routing), (weight_h, weight), (gate_h, gate), (gain_h, gain),
            (residual_h, residual), (ffn_gain_h, ffn_gain),
        ))
    ]
    for move in moves:
        move.start()
    barrier = greet(n)
    w_copy = pltpu.make_async_copy(w_hbm, w_out, w_sem)
    homes = ((g_hbm, wg), (u_hbm, wu), (d_hbm, wd))
    local = [
        pltpu.make_async_copy(src.at[0], dst.at[0], l_sem.at[i])
        for i, (src, dst) in enumerate(homes)
    ]
    peer = [
        pltpu.make_async_remote_copy(
            src_ref=src.at[0], dst_ref=dst.at[1],
            send_sem=ps_sem.at[i], recv_sem=pr_sem.at[i],
            device_id={"tp": 1 - core}, device_id_type=MESH,
        )
        for i, (src, dst) in enumerate(homes)
    ]
    w_copy.start()
    for copy in local:
        copy.start()
    for move in moves[:4]:
        move.wait()

    row = lax.broadcasted_iota(jnp.int32, (length, length), 0)
    col = lax.broadcasted_iota(jnp.int32, (length, length), 1)
    causal = row >= col
    tri = causal.astype(f32)
    def owned(g, index):
        return pl.ds(pl.multiple_of(g * per * HEAD_DIM + index * piece, piece), piece)

    def state_copy(g, r):
        return pltpu.make_async_remote_copy(
            src_ref=st_send.at[owned(g, partner(me, r))], dst_ref=st_recv.at[g, r],
            send_sem=s_sem.at[g, r], recv_sem=r_sem.at[g, r],
            device_id={"sp": partner(me, r)}, device_id_type=MESH,
        )

    def decay_copy(g, r):
        return pltpu.make_async_remote_copy(
            src_ref=dec_send.at[g], dst_ref=dec_recv.at[g, r],
            send_sem=ds_sem.at[g, r], recv_sem=dr_sem.at[g, r],
            device_id={"sp": partner(me, r)}, device_id_type=MESH,
        )

    def back_copy(g, r):
        return pltpu.make_async_remote_copy(
            src_ref=ret_send.at[g, partner(me, r)], dst_ref=ret_recv.at[owned(g, me)],
            send_sem=bs_sem.at[g, r], recv_sem=br_sem.at[g, r],
            device_id={"sp": partner(me, r)}, device_id_type=MESH,
        )

    def back_from(g, r):
        return pltpu.make_async_remote_copy(
            src_ref=ret_send.at[g, me], dst_ref=ret_recv.at[owned(g, partner(me, r))],
            send_sem=bs_sem.at[g, r], recv_sem=br_sem.at[g, r],
            device_id={"sp": partner(me, r)}, device_id_type=MESH,
        )

    others = range(n - 1, 0, -1)

    for h in range(heads):
        c = slice(h * HEAD_DIM, (h + 1) * HEAD_DIM)
        key = (1.0 - bound[:, c]) / (1.0 + jnp.exp(logit[:, c].astype(f32)))
        cum = dot(tri, jnp.log1p(-key), precision=lax.Precision.HIGHEST)
        last = cum[length - 1 :, :]
        mid_cum = 0.5 * last
        q_scr[:, c] = (query[:, c].astype(f32) * jnp.exp(cum - mid_cum)).astype(bf16)
        keys = (key * jnp.exp(mid_cum - cum)).astype(bf16)
        k_scr[:, c] = keys
        st_send[c, :] = (dot(value[:, c], keys, TN) * jnp.exp(mid_cum)).astype(bf16)
        dec_send[h // per, h % per : h % per + 1, :] = last

    plane = n // 4
    z, spot = me // plane, me % plane
    upper = z // 2
    first_near = 2 * upper * plane
    is_mid = z == 1 + upper
    far_mid, far_end = 2 - upper, 3 - 3 * upper
    my_kind = jnp.where(is_mid, 0, 1)
    near = 2 * plane
    near_slots = near * cap

    for move in moves[4:]:
        move.wait()
    top, count = routing.shape
    owner = lax.broadcasted_iota(jnp.int32, (n, count), 0)
    before = (
        lax.broadcasted_iota(jnp.int32, (count, count), 0)
        < lax.broadcasted_iota(jnp.int32, (count, count), 1)
    ).astype(bf16)
    used = jnp.zeros((n, 1), f32)
    slot_rows, weight_rows = [], []
    for k in range(top):
        hot = (routing[k : k + 1, :] == owner).astype(f32)
        rank = dot(hot.astype(bf16), before) + used
        used = used + jnp.sum(hot, axis=1, keepdims=True)
        slot_rows.append(
            jnp.sum(hot * (rank + owner.astype(f32) * cap), axis=0, keepdims=True)
        )
        weight_rows.append(weight[k : k + 1, :])

    def tables(index, slots, weights):
        line = lax.broadcasted_iota(jnp.int32, (near_slots, count), 0).astype(f32)
        chosen = jnp.zeros((near_slots, count), f32)
        scale = jnp.zeros((near_slots, count), f32)
        for slot, share in zip(slots, weights):
            mine = slot == line
            chosen = jnp.where(mine, 1.0, chosen)
            scale = jnp.where(mine, share, scale)
        high = scale.astype(bf16)
        pick[index] = chosen.astype(bf16)
        comb[index, 0] = high
        comb[index, 1] = (scale - high.astype(f32)).astype(bf16)

    def base_of(first):
        return (first * cap).astype(f32)

    tables(0, [slot - base_of(first_near) for slot in slot_rows], weight_rows)
    info_send[...] = jnp.zeros_like(info_send)
    for k in range(top):
        info_send[k : k + 1, :count] = slot_rows[k] - base_of(near - first_near)
        info_send[top + k : top + k + 1, :count] = weight_rows[k]

    pl.semaphore_wait(barrier, n)
    for g in range(groups):
        for r in others:
            decay_copy(g, r).start()
            state_copy(g, r).start()
    info_copy = pltpu.make_async_remote_copy(
        src_ref=info_send, dst_ref=info_recv.at[my_kind],
        send_sem=is_sem, recv_sem=ir_sem.at[my_kind],
        device_id={"sp": far_mid * plane + spot}, device_id_type=MESH,
    )
    info_copy.start()
    for copy in peer:
        copy.start()
    for g in range(groups):
        st_recv[g, 0] = st_send[owned(g, me), :]
        dec_recv[g, 0] = dec_send[g]

    for h in range(heads):
        c = slice(h * HEAD_DIM, (h + 1) * HEAD_DIM)
        scores = jnp.where(causal, dot(q_scr[:, c], k_scr[:, c], NT), 0.0).astype(bf16)
        ho[:, c] = dot(scores, value[:, c])
        g = gate[:, c].astype(f32)
        gated[:, c] = gain[:, c] * (g / (1.0 + jnp.exp(-g)))

    @pl.when(is_mid)
    def _():
        for kind in range(2):
            pltpu.make_async_remote_copy(
                src_ref=info_send, dst_ref=info_recv.at[kind],
                send_sem=is_sem, recv_sem=ir_sem.at[kind],
                device_id={"sp": far_mid * plane + spot}, device_id_type=MESH,
            ).wait_recv()
            tables(
                1 + kind,
                [info_recv[kind, k : k + 1, :count] for k in range(top)],
                [info_recv[kind, top + k : top + k + 1, :count] for k in range(top)],
            )

    own_head = me * piece // HEAD_DIM
    for g in range(groups):
        for r in others:
            decay_copy(g, r).wait_recv()
            state_copy(g, r).wait_recv()

        def prefix(p, acc):
            r = 0
            step = 1
            while step < n:
                r = r + step * ((me // step + p // step) % 2)
                step *= 2
            last = dec_recv[g, r, pl.ds(own_head, 1), :]
            ret_send[g, p] = (acc * jnp.exp(0.5 * last)).astype(bf16)
            return acc * jnp.exp(last) + st_recv[g, r].astype(f32)

        lax.fori_loop(0, n, prefix, jnp.zeros((piece, HEAD_DIM), f32), unroll=n <= 16)
        for r in others:
            back_copy(g, r).start()
        ret_recv[owned(g, me), :] = ret_send[g, me]

    for h in range(heads):
        c = slice(h * HEAD_DIM, (h + 1) * HEAD_DIM)
        if h % per == 0:
            for r in others:
                back_from(h // per, r).wait_recv()
        out = ho[:, c] + dot(q_scr[:, c], ret_recv[c, :], NT)
        out = out * lax.rsqrt(jnp.mean(out * out, axis=1, keepdims=True) + epsilon)
        out = (out * gated[:, c]).astype(bf16)
        mixed[0, :, c] = out[:half]
        mixed[1, :, c] = out[half:]

    swap = pltpu.make_async_remote_copy(
        src_ref=mixed.at[1 - core], dst_ref=regrouped,
        send_sem=ms_sem, recv_sem=mr_sem,
        device_id={"tp": 1 - core}, device_id_type=MESH,
    )
    swap.start()
    w_copy.wait()
    tile = 512
    total = w_out.shape[1]

    def project(which, source, first):
        @pl.loop(0, total // tile)
        def _(j):
            cols = pl.ds(pl.multiple_of(j * tile, tile), tile)
            part = dot(source, w_out[rows_of(which, width), cols])
            proj[:, cols] = part if first else proj[:, cols] + part

    project(core, mixed[core], True)
    swap.wait()
    project(1 - core, regrouped[...], False)
    updated = (residual[...].astype(f32) + proj[...]).astype(bf16)
    updated = updated.astype(f32)
    proj[...] = updated
    normed[...] = (
        updated
        * lax.rsqrt(jnp.mean(updated * updated, axis=1, keepdims=True) + epsilon)
        * ffn_gain[...]
    ).astype(bf16)

    chunks = 2
    wide = total // chunks

    def part_of(k):
        return pl.ds(k * wide, wide)

    def dense_copy(kind, k, relay):
        return pltpu.make_async_remote_copy(
            src_ref=normed.at[:, part_of(k)], dst_ref=dense_in.at[kind, :, part_of(k)],
            send_sem=vs_sem.at[k], recv_sem=vr_sem.at[kind, k],
            device_id={"sp": relay * plane + spot}, device_id_type=MESH,
        )

    def block(r):
        return pl.ds(r * cap, cap)

    def local_rows(device):
        return rows_of(device - first_near, cap)

    def send_copy(r):
        return pltpu.make_async_remote_copy(
            src_ref=outbox.at[local_rows(partner(me, r))], dst_ref=arrived.at[block(r)],
            send_sem=xs_sem.at[r], recv_sem=xr_sem.at[r],
            device_id={"sp": partner(me, r)}, device_id_type=MESH,
        )

    def relay_copy(kind, r, k):
        return pltpu.make_async_remote_copy(
            src_ref=relay_out.at[kind, local_rows(partner(me, r)), part_of(k)],
            dst_ref=arrived.at[block(near + kind * plane + r % plane), part_of(k)],
            send_sem=fs_sem.at[kind, r, k], recv_sem=fr_sem.at[kind, r % plane, k],
            device_id={"sp": partner(me, r)}, device_id_type=MESH,
        )

    def relay_from(kind, r, k):
        return pltpu.make_async_remote_copy(
            src_ref=relay_out.at[kind, local_rows(partner(me, r)), part_of(k)],
            dst_ref=arrived.at[block(near + kind * plane + r), part_of(k)],
            send_sem=fs_sem.at[kind, r, k], recv_sem=fr_sem.at[kind, r, k],
            device_id={"sp": (1 + upper) * plane + partner(spot, r)}, device_id_type=MESH,
        )

    def answer_copy(r):
        return pltpu.make_async_remote_copy(
            src_ref=result.at[block(r)], dst_ref=returned.at[local_rows(me)],
            send_sem=ys_sem.at[r], recv_sem=yr_sem.at[r],
            device_id={"sp": partner(me, r)}, device_id_type=MESH,
        )

    def answer_from(r):
        return pltpu.make_async_remote_copy(
            src_ref=result.at[block(r)], dst_ref=returned.at[local_rows(partner(me, r))],
            send_sem=ys_sem.at[r], recv_sem=yr_sem.at[r],
            device_id={"sp": partner(me, r)}, device_id_type=MESH,
        )

    def gather_copy(kind, r, k):
        return pltpu.make_async_remote_copy(
            src_ref=result.at[block(near + kind * plane + r), part_of(k)],
            dst_ref=relay_in.at[kind, local_rows(me), part_of(k)],
            send_sem=gs_sem.at[kind, r, k], recv_sem=gr_sem.at[kind, my_kind * plane + r, k],
            device_id={"sp": (1 + upper) * plane + partner(spot, r)}, device_id_type=MESH,
        )

    def gather_from(kind, r, k):
        return pltpu.make_async_remote_copy(
            src_ref=result.at[block(near + kind * plane + r % plane), part_of(k)],
            dst_ref=relay_in.at[kind, local_rows(partner(me, r)), part_of(k)],
            send_sem=gs_sem.at[kind, r % plane, k], recv_sem=gr_sem.at[kind, r, k],
            device_id={"sp": partner(me, r)}, device_id_type=MESH,
        )

    def home_copy(kind, k):
        return pltpu.make_async_remote_copy(
            src_ref=dense_out.at[kind, :, part_of(k)], dst_ref=dense_ret.at[:, part_of(k)],
            send_sem=es_sem.at[kind, k], recv_sem=er_sem.at[k],
            device_id={"sp": (far_mid, far_end)[kind] * plane + spot}, device_id_type=MESH,
        )

    @pl.when(is_mid)
    def _():
        for k in range(chunks):
            dense_copy(0, k, far_mid).start()

    outbox[...] = dot(pick[0], normed[...]).astype(bf16)
    for r in range(near - 1, plane - 1, -1):
        send_copy(r).start()

    @pl.when(jnp.logical_not(is_mid))
    def _():
        for k in range(chunks):
            dense_copy(1, k, far_mid).start()

    for r in range(plane - 1, 0, -1):
        send_copy(r).start()
    arrived[block(0), :] = outbox[local_rows(me), :]

    def relay(kind):
        @pl.when(is_mid)
        def _():
            for k in range(chunks):
                dense_copy(kind, k, far_mid).wait_recv()
                relay_out[kind, :, part_of(k)] = dot(
                    pick[1 + kind], dense_in[kind, :, part_of(k)]
                ).astype(bf16)
                for r in range(near - 1, 0, -1):
                    relay_copy(kind, r, k).start()
                arrived[block(near + kind * plane), part_of(k)] = relay_out[
                    kind, local_rows(me), part_of(k)
                ]

    inner = wg.shape[2]
    narrow = 256

    def raise_up(part):
        for s in range(2):

            @pl.loop(0, inner // narrow)
            def _(j):
                cols = rows_of(j, narrow)
                g = dot(arrived[part, :], wg[s, :, cols])
                u = dot(arrived[part, :], wu[s, :, cols])
                hidden[s, part, cols] = (g / (1.0 + jnp.exp(-g)) * u).astype(bf16)

    def bring_down(part, k):
        @pl.loop(0, wide // tile)
        def _(j):
            cols = pl.ds(pl.multiple_of(k * wide + j * tile, tile), tile)
            result[part, cols] = (
                dot(hidden[0, part, :], wd[0, :, cols]) + dot(hidden[1, part, :], wd[1, :, cols])
            ).astype(bf16)

    def far_group(kind):
        for r in range(plane):
            for k in range(chunks):
                if r:
                    relay_from(kind, r, k).wait_recv()
                else:

                    @pl.when(jnp.logical_not(is_mid))
                    def _():
                        relay_from(kind, r, k).wait_recv()

        part = slice((near + kind * plane) * cap, (near + (kind + 1) * plane) * cap)
        raise_up(part)
        for k in range(chunks):
            bring_down(part, k)
            for r in range(plane - 1, 0, -1):
                gather_copy(kind, r, k).start()

            @pl.when(jnp.logical_not(is_mid))
            def _():
                gather_copy(kind, 0, k).start()

            @pl.when(is_mid)
            def _():
                relay_in[kind, local_rows(me), part_of(k)] = result[
                    block(near + kind * plane), part_of(k)
                ]

    relay(0)
    for copy in peer + local:
        copy.wait()
    for r in range(1, near):
        send_copy(r).wait_recv()
    raise_up(slice(0, near_slots))
    for k in range(chunks):
        bring_down(slice(0, near_slots), k)
    for r in range(near - 1, 0, -1):
        answer_copy(r).start()
    returned[local_rows(me), :] = result[block(0), :]
    relay(1)
    far_group(0)
    far_group(1)

    @pl.when(is_mid)
    def _():
        for kind in range(2):
            for k in range(chunks):
                for r in range(1, near):
                    gather_from(kind, r, k).wait_recv()
                rows = relay_in[kind, :, part_of(k)]
                dense_out[kind, :, part_of(k)] = (
                    dot(comb[1 + kind, 0], rows, TN) + dot(comb[1 + kind, 1], rows, TN)
                ).astype(bf16)
                home_copy(kind, k).start()

    for r in range(1, near):
        answer_from(r).wait_recv()

    @pl.loop(0, total // tile)
    def _(j):
        cols = rows_of(j, tile)
        rows = returned[:, cols]
        proj[:, cols] = proj[:, cols] + (dot(comb[0, 0], rows, TN) + dot(comb[0, 1], rows, TN))

    for k in range(chunks):
        home_copy(0, k).wait_recv()
        layer_out[:, part_of(k)] = (
            proj[:, part_of(k)] + dense_ret[:, part_of(k)].astype(f32)
        ).astype(bf16)

    for g in range(groups):
        for r in others:
            decay_copy(g, r).wait_send()
            state_copy(g, r).wait_send()
            back_copy(g, r).wait_send()

    info_copy.wait_send()
    for k in range(chunks):
        dense_copy(0, k, far_mid).wait_send()
    for r in range(1, near):
        send_copy(r).wait_send()
        answer_copy(r).wait_send()
    for kind in range(2):
        for k in range(chunks):
            for r in range(1, plane):
                gather_copy(kind, r, k).wait_send()

            @pl.when(jnp.logical_not(is_mid))
            def _():
                gather_copy(kind, 0, k).wait_send()

            @pl.when(is_mid)
            def _():
                for r in range(1, near):
                    relay_copy(kind, r, k).wait_send()
                home_copy(kind, k).wait_send()


def solution(mesh):
    n = mesh.shape["sp"]
    vmem = pl.BlockSpec(memory_space=pltpu.VMEM)
    hbm = pl.BlockSpec(memory_space=pl.ANY)
    dma = pltpu.SemaphoreType.DMA

    def body(
        query, forget_logit, value, out_gate, lower_bound, head_gain, residual_in, w_out,
        ffn_gain, routing, route_weight, expert_gate, expert_up, expert_down,
    ):
        length, width = query.shape
        heads = width // HEAD_DIM
        half, model = residual_in.shape
        cap = 2 * half * routing.shape[1] // n
        cap = -(-cap // 16) * 16
        plane = n // 4
        near = 2 * plane
        slots, near_slots = n * cap, near * cap
        chunks = 2
        groups = 2 if heads % 2 == 0 and width // n % 32 == 0 else 1
        piece = width // n // groups
        inner = expert_gate.shape[2]
        top = routing.shape[1]
        return pl.pallas_call(
            functools.partial(layer_kernel, n, cap),
            out_shape=jax.ShapeDtypeStruct((half, model), bf16),
            in_specs=[hbm] * 14,
            out_specs=vmem,
            scratch_shapes=[
                pltpu.VMEM((length, width), bf16),
                pltpu.VMEM((length, width), bf16),
                pltpu.VMEM((length, width), bf16),
                pltpu.VMEM((length, width), bf16),
                pltpu.VMEM((1, width), f32),
                pltpu.VMEM((1, width), f32),
                pltpu.VMEM((half, model), bf16),
                pltpu.VMEM((1, model), f32),
                pltpu.VMEM((top, half), jnp.int32),
                pltpu.VMEM((top, half), f32),
                pltpu.VMEM(w_out.shape, bf16),
                pltpu.VMEM((length, width), bf16),
                pltpu.VMEM((length, width), bf16),
                pltpu.VMEM((length, width), f32),
                pltpu.VMEM((width, HEAD_DIM), bf16),
                pltpu.VMEM((groups, n, piece, HEAD_DIM), bf16),
                pltpu.VMEM((groups, heads // groups, HEAD_DIM), f32),
                pltpu.VMEM((groups, n, heads // groups, HEAD_DIM), f32),
                pltpu.VMEM((groups, n, piece, HEAD_DIM), bf16),
                pltpu.VMEM((width, HEAD_DIM), bf16),
                pltpu.VMEM((2, half, width), bf16),
                pltpu.VMEM((half, width), bf16),
                pltpu.VMEM((half, model), f32),
                pltpu.VMEM((2, model, inner), bf16),
                pltpu.VMEM((2, model, inner), bf16),
                pltpu.VMEM((2, inner, model), bf16),
                pltpu.VMEM((length, width), f32),
                pltpu.VMEM((half, model), bf16),
                pltpu.VMEM((3, near_slots, half), bf16),
                pltpu.VMEM((3, 2, near_slots, half), bf16),
                pltpu.VMEM((-(-2 * top // 8) * 8, -(-half // 128) * 128), f32),
                pltpu.VMEM((2, -(-2 * top // 8) * 8, -(-half // 128) * 128), f32),
                pltpu.VMEM((near_slots, model), bf16),
                pltpu.VMEM((slots, model), bf16),
                pltpu.VMEM((2, slots, inner), bf16),
                pltpu.VMEM((slots, model), bf16),
                pltpu.VMEM((near_slots, model), bf16),
                pltpu.VMEM((2, half, model), bf16),
                pltpu.VMEM((2, near_slots, model), bf16),
                pltpu.VMEM((2, near_slots, model), bf16),
                pltpu.VMEM((2, half, model), bf16),
                pltpu.VMEM((half, model), bf16),
                dma((10,)), dma,
                dma((groups, n)), dma((groups, n)), dma((groups, n)),
                dma((groups, n)), dma((groups, n)), dma((groups, n)),
                dma, dma, dma((3,)), dma((3,)), dma((3,)),
                dma, dma((2,)),
                dma((near,)), dma((near,)), dma((near,)), dma((near,)),
                dma((chunks,)), dma((2, chunks)),
                dma((2, near, chunks)), dma((2, plane, chunks)),
                dma((2, plane, chunks)), dma((2, near, chunks)),
                dma((2, chunks)), dma((chunks,)),
            ],
            compiler_params=pltpu.CompilerParams(
                collective_id=0, has_side_effects=True, vmem_limit_bytes=60 << 20
            ),
        )(
            query, forget_logit, value, out_gate, lower_bound[None], head_gain[None],
            residual_in, ffn_gain[None], routing.T, route_weight.T, w_out,
            expert_gate, expert_up, expert_down,
        )

    placed = (
        P("sp", "tp"), P("sp", "tp"), P("sp", "tp"), P("sp", "tp"), P("tp"), P("tp"),
        P(("sp", "tp"), None), P(), P(), P(("sp", "tp"), None), P(("sp", "tp"), None),
        P("sp", None, "tp"), P("sp", None, "tp"), P("sp", "tp", None),
    )
    return jax.shard_map(
        body, mesh=mesh, in_specs=placed, out_specs=P(("sp", "tp"), None), check_vma=False
    )
```

```python
import functools

import jax
import jax.numpy as jnp
from jax import lax
from jax.experimental import pallas as pl
from jax.experimental.pallas import tpu as pltpu
from jax.sharding import PartitionSpec as P

HEAD_DIM = 128
MESH = pl.DeviceIdType.MESH
epsilon = 1e-06
f32 = jnp.float32
bf16 = jnp.bfloat16
NT = (((1,), (1,)), ((), ()))
TN = (((0,), (0,)), ((), ()))


def dot(a, b, dims=(((1,), (0,)), ((), ())), precision=None):
    return lax.dot_general(a, b, dims, precision=precision, preferred_element_type=f32)


def rows_of(index, count):
    return pl.ds(pl.multiple_of(index * count, count), count)


def greet(n):
    me, core = lax.axis_index("sp"), lax.axis_index("tp")
    barrier = pltpu.get_barrier_semaphore()
    pl.semaphore_signal(barrier, inc=1, device_id={"tp": 1 - core}, device_id_type=MESH)

    @pl.loop(1, n)
    def _(r):
        pl.semaphore_signal(
            barrier, inc=1, device_id={"sp": lax.rem(me + r, n)}, device_id_type=MESH
        )

    return barrier


def partner(me, r):
    other = me
    step = 1
    while step <= r:
        if r & step:
            other = other + step * (1 - 2 * (me // step % 2))
        step *= 2
    return other


def arrivals(ref, sem):
    peer = {"tp": 1 - lax.axis_index("tp")}
    pltpu.make_async_remote_copy(ref, ref, sem, sem, device_id=peer, device_id_type=MESH).wait_recv()


def departures(ref, sem):
    peer = {"tp": 1 - lax.axis_index("tp")}
    pltpu.make_async_remote_copy(ref, ref, sem, sem, device_id=peer, device_id_type=MESH).wait_send()


def layer_kernel(
    n, cap,
    query_h, logit_h, value_h, gate_h, bound_h, gain_h, residual_h, ffn_gain_h, routing_h,
    weight_h, w_hbm, g_hbm, u_hbm, d_hbm,
    layer_out,
    query, logit, value, gate, bound, gain, residual, ffn_gain, routing, weight,
    w_out, q_scr, k_scr, ho, st_send, st_recv, dec_send, dec_recv, ret_send, ret_recv,
    mixed, regrouped, proj,
    wg, wu, wd, gated, normed, pick, comb, pick_far, comb_far, info_send, info_recv,
    outbox, arrived, acc, hidden, result, returned, dense_in, far_out, part_in, part_add, dense_out, dense_ret,
    in_sem, w_sem, s_sem, r_sem, ds_sem, dr_sem, bs_sem, br_sem, ms_sem, mr_sem,
    l_sem, ps_sem, pr_sem, is_sem, ir_sem, xs_sem, xr_sem, ys_sem, yr_sem,
    vs_sem, vr_sem, ws_sem, fs_sem, fr_sem, gs_sem, gr_sem, as_sem, ar_sem, es_sem, er_sem,
):
    me, core = lax.axis_index("sp"), lax.axis_index("tp")
    length, width = query.shape
    heads = width // HEAD_DIM
    groups, piece = st_recv.shape[0], st_recv.shape[2]
    per = heads // groups
    half = length // 2
    moves = [
        pltpu.make_async_copy(src, dst, in_sem.at[i])
        for i, (src, dst) in enumerate((
            (logit_h, logit), (bound_h, bound), (query_h, query), (value_h, value),
            (routing_h, routing), (weight_h, weight), (gate_h, gate), (gain_h, gain),
            (residual_h, residual), (ffn_gain_h, ffn_gain),
        ))
    ]
    for move in moves:
        move.start()
    barrier = greet(n)
    w_copy = pltpu.make_async_copy(w_hbm, w_out, w_sem)
    homes = ((g_hbm, wg), (u_hbm, wu), (d_hbm, wd))
    local = [
        pltpu.make_async_copy(src.at[0], dst.at[0], l_sem.at[i])
        for i, (src, dst) in enumerate(homes)
    ]
    peer = [
        pltpu.make_async_remote_copy(
            src_ref=src.at[0], dst_ref=dst.at[1],
            send_sem=ps_sem.at[i], recv_sem=pr_sem.at[i],
            device_id={"tp": 1 - core}, device_id_type=MESH,
        )
        for i, (src, dst) in enumerate(homes)
    ]
    w_copy.start()
    for copy in local:
        copy.start()
    for move in moves[:4]:
        move.wait()

    row = lax.broadcasted_iota(jnp.int32, (length, length), 0)
    col = lax.broadcasted_iota(jnp.int32, (length, length), 1)
    causal = row >= col
    tri = causal.astype(f32)
    def owned(g, index):
        return pl.ds(pl.multiple_of(g * per * HEAD_DIM + index * piece, piece), piece)

    def state_copy(g, r):
        return pltpu.make_async_remote_copy(
            src_ref=st_send.at[owned(g, partner(me, r))], dst_ref=st_recv.at[g, r],
            send_sem=s_sem, recv_sem=r_sem.at[g],
            device_id={"sp": partner(me, r)}, device_id_type=MESH,
        )

    def decay_copy(g, r):
        return pltpu.make_async_remote_copy(
            src_ref=dec_send.at[g], dst_ref=dec_recv.at[g, r],
            send_sem=ds_sem, recv_sem=dr_sem.at[g],
            device_id={"sp": partner(me, r)}, device_id_type=MESH,
        )

    def back_copy(g, r):
        return pltpu.make_async_remote_copy(
            src_ref=ret_send.at[g, partner(me, r)], dst_ref=ret_recv.at[owned(g, me)],
            send_sem=bs_sem, recv_sem=br_sem.at[g],
            device_id={"sp": partner(me, r)}, device_id_type=MESH,
        )

    others = range(n - 1, 0, -1)

    for h in range(heads):
        c = slice(h * HEAD_DIM, (h + 1) * HEAD_DIM)
        key = (1.0 - bound[:, c]) / (1.0 + jnp.exp(logit[:, c].astype(f32)))
        cum = dot(tri, jnp.log1p(-key), precision=lax.Precision.HIGHEST)
        last = cum[length - 1 :, :]
        mid_cum = 0.5 * last
        q_scr[:, c] = (query[:, c].astype(f32) * jnp.exp(cum - mid_cum)).astype(bf16)
        keys = (key * jnp.exp(mid_cum - cum)).astype(bf16)
        k_scr[:, c] = keys
        st_send[c, :] = (dot(value[:, c], keys, TN) * jnp.exp(mid_cum)).astype(bf16)
        dec_send[h // per, h % per : h % per + 1, :] = last

    plane = n // 4
    z, spot = me // plane, me % plane
    upper = z // 2
    first_near = 2 * upper * plane
    is_mid = z == 1 + upper
    far_mid, far_end = 2 - upper, 3 - 3 * upper
    my_kind = jnp.where(is_mid, 0, 1)
    near = 2 * plane
    near_slots = near * cap

    for move in moves[4:]:
        move.wait()
    top, count = routing.shape
    owner = lax.broadcasted_iota(jnp.int32, (n, count), 0)
    before = (
        lax.broadcasted_iota(jnp.int32, (count, count), 0)
        < lax.broadcasted_iota(jnp.int32, (count, count), 1)
    ).astype(bf16)
    used = jnp.zeros((n, 1), f32)
    slot_rows, weight_rows = [], []
    for k in range(top):
        hot = (routing[k : k + 1, :] == owner).astype(f32)
        rank = dot(hot.astype(bf16), before) + used
        used = used + jnp.sum(hot, axis=1, keepdims=True)
        slot_rows.append(
            jnp.sum(hot * (rank + owner.astype(f32) * cap), axis=0, keepdims=True)
        )
        weight_rows.append(weight[k : k + 1, :])

    eye = lax.broadcasted_iota(jnp.int32, (count, count), 0) == lax.broadcasted_iota(
        jnp.int32, (count, count), 1
    )

    def column(line):
        return jnp.sum(jnp.where(eye, line, 0.0), axis=1, keepdims=True)

    def tables(chosen_ref, scale_ref, slots, weights):
        lines = chosen_ref.shape[0]
        down = lax.broadcasted_iota(jnp.int32, (lines, count), 0).astype(f32)
        across = lax.broadcasted_iota(jnp.int32, (count, lines), 1).astype(f32)
        chosen = jnp.zeros((lines, count), f32)
        scale = jnp.zeros((count, lines), f32)
        for slot, share in zip(slots, weights):
            chosen = jnp.where(slot == down, 1.0, chosen)
            scale = jnp.where(column(slot) == across, column(share), scale)
        high = scale.astype(bf16)
        chosen_ref[...] = chosen.astype(bf16)
        scale_ref[:count, :] = high
        scale_ref[count:, :] = (scale - high.astype(f32)).astype(bf16)

    def combined(scale, rows):
        both = dot(scale, rows)
        return both[:count] + both[count:]

    def base_of(first):
        return (first * cap).astype(f32)

    tables(pick, comb, [slot - base_of(first_near) for slot in slot_rows], weight_rows)
    info_send[...] = jnp.zeros_like(info_send)
    for k in range(top):
        info_send[k : k + 1, :count] = slot_rows[k]
        info_send[top + k : top + k + 1, :count] = weight_rows[k]

    pl.semaphore_wait(barrier, n)
    for g in range(groups):
        for r in others:
            decay_copy(g, r).start()
            state_copy(g, r).start()
    info_copies = [
        pltpu.make_async_remote_copy(
            src_ref=info_send, dst_ref=info_recv.at[my_kind],
            send_sem=is_sem, recv_sem=ir_sem.at[my_kind],
            device_id={"sp": to * plane + spot}, device_id_type=MESH,
        )
        for i, to in enumerate((far_mid, far_end))
    ]
    for copy in info_copies:
        copy.start()
    for copy in peer:
        copy.start()
    for g in range(groups):
        st_recv[g, 0] = st_send[owned(g, me), :]
        dec_recv[g, 0] = dec_send[g]

    for h in range(heads):
        c = slice(h * HEAD_DIM, (h + 1) * HEAD_DIM)
        scores = jnp.where(causal, dot(q_scr[:, c], k_scr[:, c], NT), 0.0).astype(bf16)
        ho[:, c] = dot(scores, value[:, c])
        g = gate[:, c].astype(f32)
        gated[:, c] = gain[:, c] * (g / (1.0 + jnp.exp(-g)))

    for kind in range(2):
        pltpu.make_async_remote_copy(
            src_ref=info_send, dst_ref=info_recv.at[kind],
            send_sem=is_sem, recv_sem=ir_sem.at[kind],
            device_id={"sp": far_mid * plane + spot}, device_id_type=MESH,
        ).wait_recv()
        tables(
            pick_far.at[kind],
            comb_far.at[kind],
            [info_recv[kind, k : k + 1, :count] - base_of(z * plane) for k in range(top)],
            [info_recv[kind, top + k : top + k + 1, :count] for k in range(top)],
        )

    own_head = me * piece // HEAD_DIM
    for g in range(groups):
        arrivals(dec_recv.at[g, pl.ds(1, n - 1)], dr_sem.at[g])
        arrivals(st_recv.at[g, pl.ds(1, n - 1)], r_sem.at[g])

        def prefix(p, acc):
            r = 0
            step = 1
            while step < n:
                r = r + step * ((me // step + p // step) % 2)
                step *= 2
            last = dec_recv[g, r, pl.ds(own_head, 1), :]
            ret_send[g, p] = (acc * jnp.exp(0.5 * last)).astype(bf16)
            return acc * jnp.exp(last) + st_recv[g, r].astype(f32)

        lax.fori_loop(0, n, prefix, jnp.zeros((piece, HEAD_DIM), f32), unroll=n <= 16)
        for r in others:
            back_copy(g, r).start()
        ret_recv[owned(g, me), :] = ret_send[g, me]

    total = w_out.shape[1]
    tile = 512
    band = per * HEAD_DIM

    def swap_copy(g):
        return pltpu.make_async_remote_copy(
            src_ref=mixed.at[1 - core, :, pl.ds(g * band, band)],
            dst_ref=regrouped.at[:, pl.ds(g * band, band)],
            send_sem=ms_sem, recv_sem=mr_sem.at[g],
            device_id={"tp": 1 - core}, device_id_type=MESH,
        )

    def project(which, source, g, first=False):
        depth = pl.ds(pl.multiple_of(which * width + g * band, band), band)
        for j in range(total // tile):
            cols = slice(j * tile, (j + 1) * tile)
            part = dot(source, w_out[depth, cols])
            proj[:, cols] = part if first else proj[:, cols] + part

    for g in range(groups):
        arrivals(ret_recv.at[pl.ds(g * band, (n - 1) * piece)], br_sem.at[g])
        for h in range(g * per, (g + 1) * per):
            c = slice(h * HEAD_DIM, (h + 1) * HEAD_DIM)
            out = ho[:, c] + dot(q_scr[:, c], ret_recv[c, :], NT)
            out = out * lax.rsqrt(jnp.mean(out * out, axis=1, keepdims=True) + epsilon)
            out = (out * gated[:, c]).astype(bf16)
            mixed[0, :, c] = out[:half]
            mixed[1, :, c] = out[half:]
        swap_copy(g).start()
        if g == 0:
            w_copy.wait()
        project(core, mixed[core, :, g * band : (g + 1) * band], g, first=g == 0)
        if g:
            swap_copy(g - 1).wait_recv()
            project(1 - core, regrouped[:, (g - 1) * band : g * band], g - 1)
    swap_copy(groups - 1).wait_recv()
    project(1 - core, regrouped[:, (groups - 1) * band :], groups - 1)
    updated = (residual[...].astype(f32) + proj[...]).astype(bf16)
    updated = updated.astype(f32)
    proj[...] = updated
    normed[...] = (
        updated
        * lax.rsqrt(jnp.mean(updated * updated, axis=1, keepdims=True) + epsilon)
        * ffn_gain[...]
    ).astype(bf16)

    chunks = vr_sem.shape[1]
    wide = total // chunks

    def part_of(k):
        return pl.ds(k * wide, wide)

    def dense_copy(kind, k, relay):
        return pltpu.make_async_remote_copy(
            src_ref=normed.at[:, part_of(k)], dst_ref=dense_in.at[kind, :, part_of(k)],
            send_sem=vs_sem, recv_sem=vr_sem.at[kind, k],
            device_id={"sp": relay * plane + spot}, device_id_type=MESH,
        )

    def block(r):
        return pl.ds(r * cap, cap)

    def local_rows(device):
        return rows_of(device - first_near, cap)

    def send_copy(r):
        return pltpu.make_async_remote_copy(
            src_ref=outbox.at[local_rows(partner(me, r))], dst_ref=arrived.at[block(r)],
            send_sem=xs_sem, recv_sem=xr_sem.at[r // plane],
            device_id={"sp": partner(me, r)}, device_id_type=MESH,
        )

    def forward_copy(kind, k):
        return pltpu.make_async_remote_copy(
            src_ref=dense_in.at[kind, :, part_of(k)], dst_ref=dense_in.at[kind, :, part_of(k)],
            send_sem=ws_sem, recv_sem=vr_sem.at[kind, k],
            device_id={"sp": partner(me, plane)}, device_id_type=MESH,
        )

    def scatter_copy(kind, r, k):
        return pltpu.make_async_remote_copy(
            src_ref=far_out.at[kind, rows_of(partner(spot, r), cap), part_of(k)],
            dst_ref=arrived.at[block(near + kind * plane + r), part_of(k)],
            send_sem=fs_sem, recv_sem=fr_sem.at[kind, k],
            device_id={"sp": partner(me, r)}, device_id_type=MESH,
        )

    def answer_copy(r, k):
        return pltpu.make_async_remote_copy(
            src_ref=result.at[block(r), part_of(k)],
            dst_ref=returned.at[local_rows(me), part_of(k)],
            send_sem=ys_sem, recv_sem=yr_sem.at[k],
            device_id={"sp": partner(me, r)}, device_id_type=MESH,
        )

    def gather_copy(kind, r, k):
        return pltpu.make_async_remote_copy(
            src_ref=result.at[block(near + kind * plane + r), part_of(k)],
            dst_ref=part_in.at[kind, rows_of(spot, cap), part_of(k)],
            send_sem=gs_sem, recv_sem=gr_sem.at[kind, k],
            device_id={"sp": partner(me, r)}, device_id_type=MESH,
        )

    def inward_copy(kind, k):
        return pltpu.make_async_remote_copy(
            src_ref=dense_out.at[kind, :, part_of(k)], dst_ref=part_add.at[kind, :, part_of(k)],
            send_sem=as_sem, recv_sem=ar_sem.at[kind, k],
            device_id={"sp": partner(me, plane)}, device_id_type=MESH,
        )

    def home_copy(kind, k):
        return pltpu.make_async_remote_copy(
            src_ref=dense_out.at[kind, :, part_of(k)], dst_ref=dense_ret.at[:, part_of(k)],
            send_sem=es_sem, recv_sem=er_sem.at[k],
            device_id={"sp": (far_mid, far_end)[kind] * plane + spot}, device_id_type=MESH,
        )

    not_mid = jnp.logical_not(is_mid)

    @pl.when(not_mid)
    def _():
        for k in range(chunks):
            dense_copy(1, k, far_mid).start()

    outbox[...] = dot(pick[...], normed[...]).astype(bf16)
    for r in range(plane - 1, 0, -1):
        send_copy(r).start()

    for r in range(near - 1, plane - 1, -1):
        send_copy(r).start()

    arrived[block(0), :] = outbox[local_rows(me), :]

    def forward(kind, k):
        @pl.when(is_mid)
        def _():
            dense_copy(kind, k, far_mid).wait_recv()
            forward_copy(kind, k).start()

    def scatter(kind, k):
        @pl.when(not_mid)
        def _():
            dense_copy(kind, k, far_mid).wait_recv()

        far_out[kind, :, part_of(k)] = dot(
            pick_far[kind], dense_in[kind, :, part_of(k)]
        ).astype(bf16)
        for r in range(plane - 1, 0, -1):
            scatter_copy(kind, r, k).start()
        arrived[block(near + kind * plane), part_of(k)] = far_out[
            kind, rows_of(spot, cap), part_of(k)
        ]

    inner = wg.shape[2]
    rows_each = plane * cap

    def rows_in(group):
        return slice(group * rows_each, (group + 1) * rows_each)

    def raise_up(group, k):
        part = rows_in(group)
        x = arrived[part, part_of(k)]
        for s in range(2):
            g = dot(x, wg[s, part_of(k), :])
            u = dot(x, wu[s, part_of(k), :])
            if k:
                g = g + acc[0, s]
                u = u + acc[1, s]
            if k < chunks - 1:
                acc[0, s] = g
                acc[1, s] = u
            else:
                hidden[s, part, :] = (g / (1.0 + jnp.exp(-g)) * u).astype(bf16)

    def bring_down(group, k):
        part = rows_in(group)
        result[part, part_of(k)] = (
            dot(hidden[0, part, :], wd[0, :, part_of(k)])
            + dot(hidden[1, part, :], wd[1, :, part_of(k)])
        ).astype(bf16)

    def near_answer(group, parts=range(4)):
        for k in parts:
            bring_down(group, k)
            for r in range((group + 1) * plane - 1, max(group * plane, 1) - 1, -1):
                answer_copy(r, k).start()
        if group == 0:
            returned[local_rows(me), :] = result[block(0), :]

    def far_arrive(kind, k):
        arrivals(
            arrived.at[pl.ds((near + kind * plane + 1) * cap, (plane - 1) * cap), part_of(k)],
            fr_sem.at[kind, k],
        )
        raise_up(2 + kind, k)

    def far_answer(kind, k):
        bring_down(2 + kind, k)
        for r in range(plane - 1, 0, -1):
            gather_copy(kind, r, k).start()
        part_in[kind, rows_of(spot, cap), part_of(k)] = result[
            block(near + kind * plane), part_of(k)
        ]

    def far_partial(kind, k):
        arrivals(
            part_in.at[kind, pl.ds(0, (plane - 1) * cap), part_of(k)], gr_sem.at[kind, k]
        )
        return combined(comb_far[kind], part_in[kind, :, part_of(k)])

    def inward(kind, k):
        @pl.when(not_mid)
        def _():
            dense_out[kind, :, part_of(k)] = far_partial(kind, k).astype(bf16)
            inward_copy(kind, k).start()

    def homeward(kind, k):
        @pl.when(is_mid)
        def _():
            mine = far_partial(kind, k)
            inward_copy(kind, k).wait_recv()
            dense_out[kind, :, part_of(k)] = (
                mine + part_add[kind, :, part_of(k)].astype(f32)
            ).astype(bf16)
            home_copy(kind, k).start()

    def start_mid():
        @pl.when(is_mid)
        def _():
            for k in range(chunks):
                dense_copy(0, k, far_mid).start()

    forward(1, 0)
    forward(1, 1)
    start_mid()
    for copy in peer + local:
        copy.wait()
    arrivals(arrived.at[pl.ds(cap, (plane - 1) * cap)], xr_sem.at[0])

    def near_raise(first):
        if first == 0:
            arrivals(arrived.at[pl.ds(plane * cap, plane * cap)], xr_sem.at[1])
        raise_up(1, first)
        raise_up(1, first + 1)

    def at_ends(step, value):
        @pl.when(not_mid)
        def _():
            step(value)

    def near_reply(first):
        near_answer(1, (first, first + 1))

    raise_up(0, 0)
    raise_up(0, 1)
    forward(1, 2)
    raise_up(0, 2)
    raise_up(0, 3)
    forward(1, 3)
    near_answer(0)
    at_ends(near_raise, 0)
    scatter(1, 0)
    at_ends(near_raise, 2)
    scatter(1, 1)
    at_ends(near_reply, 0)
    forward(0, 0)
    scatter(1, 2)
    at_ends(near_reply, 2)
    forward(0, 1)
    scatter(1, 3)
    far_arrive(1, 0)
    forward(0, 2)
    far_arrive(1, 1)
    forward(0, 3)
    far_arrive(1, 2)
    scatter(0, 0)
    far_arrive(1, 3)
    far_answer(1, 0)
    far_answer(1, 1)
    scatter(0, 1)
    far_answer(1, 2)
    far_answer(1, 3)

    @pl.when(is_mid)
    def _():
        near_raise(0)
        near_raise(2)

    scatter(0, 2)
    inward(1, 0)
    inward(1, 1)
    scatter(0, 3)
    inward(1, 2)
    inward(1, 3)

    @pl.when(is_mid)
    def _():
        near_reply(0)
        near_reply(2)

    far_arrive(0, 0)
    far_arrive(0, 1)
    far_arrive(0, 2)
    far_arrive(0, 3)
    far_answer(0, 0)
    far_answer(0, 1)
    far_answer(0, 2)
    far_answer(0, 3)
    homeward(1, 0)
    homeward(1, 1)
    homeward(1, 2)
    homeward(1, 3)
    inward(0, 0)
    inward(0, 1)
    inward(0, 2)
    inward(0, 3)
    homeward(0, 0)
    homeward(0, 1)
    homeward(0, 2)
    homeward(0, 3)
    for k in range(chunks):
        arrivals(returned.at[pl.ds(0, (near - 1) * cap), part_of(k)], yr_sem.at[k])
        home_copy(0, k).wait_recv()
        layer_out[:, part_of(k)] = (
            proj[:, part_of(k)]
            + combined(comb[...], returned[:, part_of(k)])
            + dense_ret[:, part_of(k)].astype(f32)
        ).astype(bf16)

    departures(dec_recv.at[:, pl.ds(1, n - 1)], ds_sem)
    departures(st_recv.at[:, pl.ds(1, n - 1)], s_sem)
    departures(ret_send.at[:, pl.ds(1, n - 1)], bs_sem)
    departures(info_recv, is_sem)
    departures(regrouped, ms_sem)
    departures(normed, vs_sem)
    departures(outbox.at[pl.ds(cap, (near - 1) * cap)], xs_sem)
    departures(result.at[pl.ds(cap, (near - 1) * cap)], ys_sem)
    departures(arrived.at[pl.ds(0, 2 * (plane - 1) * cap)], fs_sem)
    departures(result.at[pl.ds(0, 2 * (plane - 1) * cap)], gs_sem)

    @pl.when(not_mid)
    def _():
        departures(dense_out, as_sem)

    @pl.when(is_mid)
    def _():
        departures(dense_in, ws_sem)
        departures(dense_out, es_sem)


def solution(mesh):
    n = mesh.shape["sp"]
    vmem = pl.BlockSpec(memory_space=pltpu.VMEM)
    hbm = pl.BlockSpec(memory_space=pl.ANY)
    dma = pltpu.SemaphoreType.DMA

    def body(
        query, forget_logit, value, out_gate, lower_bound, head_gain, residual_in, w_out,
        ffn_gain, routing, route_weight, expert_gate, expert_up, expert_down,
    ):
        length, width = query.shape
        heads = width // HEAD_DIM
        half, model = residual_in.shape
        cap = 2 * half * routing.shape[1] // n
        cap = -(-cap // 16) * 16
        plane = n // 4
        near = 2 * plane
        slots, near_slots = n * cap, near * cap
        chunks = 4
        groups = max(
            g for g in (1, 2, 4) if heads % g == 0 and (g == 1 or width // n % (16 * g) == 0)
        )
        piece = width // n // groups
        inner = expert_gate.shape[2]
        top = routing.shape[1]
        return pl.pallas_call(
            functools.partial(layer_kernel, n, cap),
            out_shape=jax.ShapeDtypeStruct((half, model), bf16),
            in_specs=[hbm] * 14,
            out_specs=vmem,
            scratch_shapes=[
                pltpu.VMEM((length, width), bf16),
                pltpu.VMEM((length, width), bf16),
                pltpu.VMEM((length, width), bf16),
                pltpu.VMEM((length, width), bf16),
                pltpu.VMEM((1, width), f32),
                pltpu.VMEM((1, width), f32),
                pltpu.VMEM((half, model), bf16),
                pltpu.VMEM((1, model), f32),
                pltpu.VMEM((top, half), jnp.int32),
                pltpu.VMEM((top, half), f32),
                pltpu.VMEM(w_out.shape, bf16),
                pltpu.VMEM((length, width), bf16),
                pltpu.VMEM((length, width), bf16),
                pltpu.VMEM((length, width), f32),
                pltpu.VMEM((width, HEAD_DIM), bf16),
                pltpu.VMEM((groups, n, piece, HEAD_DIM), bf16),
                pltpu.VMEM((groups, heads // groups, HEAD_DIM), f32),
                pltpu.VMEM((groups, n, heads // groups, HEAD_DIM), f32),
                pltpu.VMEM((groups, n, piece, HEAD_DIM), bf16),
                pltpu.VMEM((width, HEAD_DIM), bf16),
                pltpu.VMEM((2, half, width), bf16),
                pltpu.VMEM((half, width), bf16),
                pltpu.VMEM((half, model), f32),
                pltpu.VMEM((2, model, inner), bf16),
                pltpu.VMEM((2, model, inner), bf16),
                pltpu.VMEM((2, inner, model), bf16),
                pltpu.VMEM((length, width), f32),
                pltpu.VMEM((half, model), bf16),
                pltpu.VMEM((near_slots, half), bf16),
                pltpu.VMEM((2 * half, near_slots), bf16),
                pltpu.VMEM((2, plane * cap, half), bf16),
                pltpu.VMEM((2, 2 * half, plane * cap), bf16),
                pltpu.VMEM((-(-2 * top // 8) * 8, -(-half // 128) * 128), f32),
                pltpu.VMEM((2, -(-2 * top // 8) * 8, -(-half // 128) * 128), f32),
                pltpu.VMEM((near_slots, model), bf16),
                pltpu.VMEM((slots, model), bf16),
                pltpu.VMEM((2, 2, plane * cap, inner), f32),
                pltpu.VMEM((2, slots, inner), bf16),
                pltpu.VMEM((slots, model), bf16),
                pltpu.VMEM((near_slots, model), bf16),
                pltpu.VMEM((2, half, model), bf16),
                pltpu.VMEM((2, plane * cap, model), bf16),
                pltpu.VMEM((2, plane * cap, model), bf16),
                pltpu.VMEM((2, half, model), bf16),
                pltpu.VMEM((2, half, model), bf16),
                pltpu.VMEM((half, model), bf16),
                dma((10,)), dma,
                dma, dma((groups,)), dma, dma((groups,)), dma, dma((groups,)),
                dma, dma((groups,)), dma((3,)), dma((3,)), dma((3,)),
                dma, dma((2,)), dma, dma((2,)), dma, dma((chunks,)),
                dma, dma((2, chunks)), dma, dma, dma((2, chunks)),
                dma, dma((2, chunks)), dma, dma((2, chunks)), dma, dma((chunks,)),
            ],
            compiler_params=pltpu.CompilerParams(
                collective_id=0, has_side_effects=True, vmem_limit_bytes=60 << 20
            ),
        )(
            query, forget_logit, value, out_gate, lower_bound[None], head_gain[None],
            residual_in, ffn_gain[None], routing.T, route_weight.T, w_out,
            expert_gate, expert_up, expert_down,
        )

    placed = (
        P("sp", "tp"), P("sp", "tp"), P("sp", "tp"), P("sp", "tp"), P("tp"), P("tp"),
        P(("sp", "tp"), None), P(), P(), P(("sp", "tp"), None), P(("sp", "tp"), None),
        P("sp", None, "tp"), P("sp", None, "tp"), P("sp", "tp", None),
    )
    return jax.shard_map(
        body, mesh=mesh, in_specs=placed, out_specs=P(("sp", "tp"), None), check_vma=False
    )
```

```python
import functools

import jax
import jax.numpy as jnp
from jax import lax
from jax.experimental import pallas as pl
from jax.experimental.pallas import tpu as pltpu
from jax.sharding import PartitionSpec as P

HEAD_DIM = 128
MESH = pl.DeviceIdType.MESH
epsilon = 1e-06
f32 = jnp.float32
bf16 = jnp.bfloat16
NT = (((1,), (1,)), ((), ()))
TN = (((0,), (0,)), ((), ()))


def dot(a, b, dims=(((1,), (0,)), ((), ())), precision=None):
    return lax.dot_general(a, b, dims, precision=precision, preferred_element_type=f32)


def rows_of(index, count):
    return pl.ds(pl.multiple_of(index * count, count), count)


def greet(n):
    me, core = lax.axis_index("sp"), lax.axis_index("tp")
    barrier = pltpu.get_barrier_semaphore()
    pl.semaphore_signal(barrier, inc=1, device_id={"tp": 1 - core}, device_id_type=MESH)

    @pl.loop(1, n)
    def _(r):
        pl.semaphore_signal(
            barrier, inc=1, device_id={"sp": lax.rem(me + r, n)}, device_id_type=MESH
        )

    return barrier


def partner(me, r):
    other = me
    step = 1
    while step <= r:
        if r & step:
            other = other + step * (1 - 2 * (me // step % 2))
        step *= 2
    return other


def arrivals(ref, sem):
    peer = {"tp": 1 - lax.axis_index("tp")}
    pltpu.make_async_remote_copy(ref, ref, sem, sem, device_id=peer, device_id_type=MESH).wait_recv()


def departures(ref, sem):
    peer = {"tp": 1 - lax.axis_index("tp")}
    pltpu.make_async_remote_copy(ref, ref, sem, sem, device_id=peer, device_id_type=MESH).wait_send()


def layer_kernel(
    n, cap,
    query_h, logit_h, value_h, gate_h, bound_h, gain_h, residual_h, ffn_gain_h, routing_h,
    weight_h, w_hbm, g_hbm, u_hbm, d_hbm,
    layer_out,
    query, logit, value, gate, bound, gain, residual, ffn_gain, routing, weight,
    w_out, q_scr, k_scr, ho, st_send, st_recv, dec_send, dec_recv, ret_send, ret_recv,
    mixed, regrouped, proj,
    wg, wu, wd, gated, normed, pick, comb, pick_far, comb_far, info_send, info_recv,
    outbox, arrived, acc, hidden, result, returned, dense_in, far_out, part_in, part_add, dense_out, dense_ret,
    in_sem, w_sem, s_sem, r_sem, ds_sem, dr_sem, bs_sem, br_sem, ms_sem, mr_sem,
    l_sem, ps_sem, pr_sem, is_sem, ir_sem, xs_sem, xr_sem, ys_sem, yr_sem,
    vs_sem, vr_sem, ws_sem, fs_sem, fr_sem, gs_sem, gr_sem, as_sem, ar_sem, es_sem, er_sem,
):
    me, core = lax.axis_index("sp"), lax.axis_index("tp")
    length, width = query.shape
    heads = width // HEAD_DIM
    groups, piece = st_recv.shape[0], st_recv.shape[2]
    per = heads // groups
    half = length // 2
    moves = [
        pltpu.make_async_copy(src, dst, in_sem.at[i])
        for i, (src, dst) in enumerate((
            (logit_h, logit), (bound_h, bound), (query_h, query), (value_h, value),
            (routing_h, routing), (weight_h, weight), (gate_h, gate), (gain_h, gain),
            (residual_h, residual), (ffn_gain_h, ffn_gain),
        ))
    ]
    for move in moves:
        move.start()
    barrier = greet(n)
    w_copy = pltpu.make_async_copy(w_hbm, w_out, w_sem)
    homes = ((g_hbm, wg), (u_hbm, wu), (d_hbm, wd))
    local = [
        pltpu.make_async_copy(src.at[0], dst.at[0], l_sem.at[i])
        for i, (src, dst) in enumerate(homes)
    ]
    peer = [
        pltpu.make_async_remote_copy(
            src_ref=src.at[0], dst_ref=dst.at[1],
            send_sem=ps_sem.at[i], recv_sem=pr_sem.at[i],
            device_id={"tp": 1 - core}, device_id_type=MESH,
        )
        for i, (src, dst) in enumerate(homes)
    ]
    w_copy.start()
    for copy in local:
        copy.start()
    for move in moves[:4]:
        move.wait()

    row = lax.broadcasted_iota(jnp.int32, (length, length), 0)
    col = lax.broadcasted_iota(jnp.int32, (length, length), 1)
    causal = row >= col
    tri = causal.astype(f32)
    def owned(g, index):
        return pl.ds(pl.multiple_of(g * per * HEAD_DIM + index * piece, piece), piece)

    def state_copy(g, r):
        return pltpu.make_async_remote_copy(
            src_ref=st_send.at[owned(g, partner(me, r))], dst_ref=st_recv.at[g, r],
            send_sem=s_sem, recv_sem=r_sem.at[g],
            device_id={"sp": partner(me, r)}, device_id_type=MESH,
        )

    def decay_copy(g, r):
        return pltpu.make_async_remote_copy(
            src_ref=dec_send.at[g], dst_ref=dec_recv.at[g, r],
            send_sem=ds_sem, recv_sem=dr_sem.at[g],
            device_id={"sp": partner(me, r)}, device_id_type=MESH,
        )

    def back_copy(g, r):
        return pltpu.make_async_remote_copy(
            src_ref=ret_send.at[g, partner(me, r)], dst_ref=ret_recv.at[owned(g, me)],
            send_sem=bs_sem, recv_sem=br_sem.at[g],
            device_id={"sp": partner(me, r)}, device_id_type=MESH,
        )

    others = range(n - 1, 0, -1)

    def local_state(h):
        c = slice(h * HEAD_DIM, (h + 1) * HEAD_DIM)
        key = (1.0 - bound[:, c]) / (1.0 + jnp.exp(logit[:, c].astype(f32)))
        cum = dot(tri, jnp.log1p(-key), precision=lax.Precision.HIGHEST)
        last = cum[length - 1 :, :]
        mid_cum = 0.5 * last
        q_scr[:, c] = (query[:, c].astype(f32) * jnp.exp(cum - mid_cum)).astype(bf16)
        keys = (key * jnp.exp(mid_cum - cum)).astype(bf16)
        k_scr[:, c] = keys
        st_send[c, :] = (dot(value[:, c], keys, TN) * jnp.exp(mid_cum)).astype(bf16)
        dec_send[h // per, h % per : h % per + 1, :] = last

    def send_states(first, last):
        for g in range(first, last):
            for r in others:
                decay_copy(g, r).start()
                state_copy(g, r).start()

    early = (groups + 1) // 2
    for h in range(early * per):
        local_state(h)
    pl.semaphore_wait(barrier, n)
    send_states(0, early)
    for h in range(early * per, heads):
        local_state(h)
    send_states(early, groups)

    plane = n // 4
    z, spot = me // plane, me % plane
    upper = z // 2
    first_near = 2 * upper * plane
    is_mid = z == 1 + upper
    far_mid, far_end = 2 - upper, 3 - 3 * upper
    my_kind = jnp.where(is_mid, 0, 1)
    near = 2 * plane
    near_slots = near * cap

    for move in moves[4:]:
        move.wait()
    top, count = routing.shape
    owner = lax.broadcasted_iota(jnp.int32, (n, count), 0)
    before = (
        lax.broadcasted_iota(jnp.int32, (count, count), 0)
        < lax.broadcasted_iota(jnp.int32, (count, count), 1)
    ).astype(bf16)
    used = jnp.zeros((n, 1), f32)
    slot_rows, weight_rows = [], []
    for k in range(top):
        hot = (routing[k : k + 1, :] == owner).astype(f32)
        rank = dot(hot.astype(bf16), before) + used
        used = used + jnp.sum(hot, axis=1, keepdims=True)
        slot_rows.append(
            jnp.sum(hot * (rank + owner.astype(f32) * cap), axis=0, keepdims=True)
        )
        weight_rows.append(weight[k : k + 1, :])

    eye = lax.broadcasted_iota(jnp.int32, (count, count), 0) == lax.broadcasted_iota(
        jnp.int32, (count, count), 1
    )

    def column(line):
        return jnp.sum(jnp.where(eye, line, 0.0), axis=1, keepdims=True)

    def tables(chosen_ref, scale_ref, slots, weights):
        lines = chosen_ref.shape[0]
        down = lax.broadcasted_iota(jnp.int32, (lines, count), 0).astype(f32)
        across = lax.broadcasted_iota(jnp.int32, (count, lines), 1).astype(f32)
        chosen = jnp.zeros((lines, count), f32)
        scale = jnp.zeros((count, lines), f32)
        for slot, share in zip(slots, weights):
            chosen = jnp.where(slot == down, 1.0, chosen)
            scale = jnp.where(column(slot) == across, column(share), scale)
        high = scale.astype(bf16)
        chosen_ref[...] = chosen.astype(bf16)
        scale_ref[:count, :] = high
        scale_ref[count:, :] = (scale - high.astype(f32)).astype(bf16)

    def combined(scale, rows):
        both = dot(scale, rows)
        return both[:count] + both[count:]

    def base_of(first):
        return (first * cap).astype(f32)

    tables(pick, comb, [slot - base_of(first_near) for slot in slot_rows], weight_rows)
    info_send[...] = jnp.zeros_like(info_send)
    for k in range(top):
        info_send[k : k + 1, :count] = slot_rows[k]
        info_send[top + k : top + k + 1, :count] = weight_rows[k]

    info_copies = [
        pltpu.make_async_remote_copy(
            src_ref=info_send, dst_ref=info_recv.at[my_kind],
            send_sem=is_sem, recv_sem=ir_sem.at[my_kind],
            device_id={"sp": to * plane + spot}, device_id_type=MESH,
        )
        for i, to in enumerate((far_mid, far_end))
    ]
    for copy in info_copies:
        copy.start()
    for copy in peer:
        copy.start()
    for g in range(groups):
        st_recv[g, 0] = st_send[owned(g, me), :]
        dec_recv[g, 0] = dec_send[g]

    for h in range(heads):
        c = slice(h * HEAD_DIM, (h + 1) * HEAD_DIM)
        scores = jnp.where(causal, dot(q_scr[:, c], k_scr[:, c], NT), 0.0).astype(bf16)
        ho[:, c] = dot(scores, value[:, c])
        g = gate[:, c].astype(f32)
        gated[:, c] = gain[:, c] * (g / (1.0 + jnp.exp(-g)))

    for kind in range(2):
        pltpu.make_async_remote_copy(
            src_ref=info_send, dst_ref=info_recv.at[kind],
            send_sem=is_sem, recv_sem=ir_sem.at[kind],
            device_id={"sp": far_mid * plane + spot}, device_id_type=MESH,
        ).wait_recv()
        tables(
            pick_far.at[kind],
            comb_far.at[kind],
            [info_recv[kind, k : k + 1, :count] - base_of(z * plane) for k in range(top)],
            [info_recv[kind, top + k : top + k + 1, :count] for k in range(top)],
        )

    own_head = me * piece // HEAD_DIM
    for g in range(groups):
        arrivals(dec_recv.at[g, pl.ds(1, n - 1)], dr_sem.at[g])
        arrivals(st_recv.at[g, pl.ds(1, n - 1)], r_sem.at[g])

        def prefix(p, acc):
            r = 0
            step = 1
            while step < n:
                r = r + step * ((me // step + p // step) % 2)
                step *= 2
            last = dec_recv[g, r, pl.ds(own_head, 1), :]
            ret_send[g, p] = (acc * jnp.exp(0.5 * last)).astype(bf16)
            return acc * jnp.exp(last) + st_recv[g, r].astype(f32)

        lax.fori_loop(0, n, prefix, jnp.zeros((piece, HEAD_DIM), f32), unroll=n <= 16)
        for r in others:
            back_copy(g, r).start()
        ret_recv[owned(g, me), :] = ret_send[g, me]

    total = w_out.shape[1]
    tile = 512
    band = per * HEAD_DIM

    def swap_copy(g):
        return pltpu.make_async_remote_copy(
            src_ref=mixed.at[1 - core, :, pl.ds(g * band, band)],
            dst_ref=regrouped.at[:, pl.ds(g * band, band)],
            send_sem=ms_sem, recv_sem=mr_sem.at[g],
            device_id={"tp": 1 - core}, device_id_type=MESH,
        )

    def project(which, source, g, first=False):
        depth = pl.ds(pl.multiple_of(which * width + g * band, band), band)
        for j in range(total // tile):
            cols = slice(j * tile, (j + 1) * tile)
            part = dot(source, w_out[depth, cols])
            proj[:, cols] = part if first else proj[:, cols] + part

    for g in range(groups):
        arrivals(ret_recv.at[pl.ds(g * band, (n - 1) * piece)], br_sem.at[g])
        for h in range(g * per, (g + 1) * per):
            c = slice(h * HEAD_DIM, (h + 1) * HEAD_DIM)
            out = ho[:, c] + dot(q_scr[:, c], ret_recv[c, :], NT)
            out = out * lax.rsqrt(jnp.mean(out * out, axis=1, keepdims=True) + epsilon)
            out = (out * gated[:, c]).astype(bf16)
            mixed[0, :, c] = out[:half]
            mixed[1, :, c] = out[half:]
        swap_copy(g).start()
        if g == 0:
            w_copy.wait()
        project(core, mixed[core, :, g * band : (g + 1) * band], g, first=g == 0)
        if g:
            swap_copy(g - 1).wait_recv()
            project(1 - core, regrouped[:, (g - 1) * band : g * band], g - 1)
    swap_copy(groups - 1).wait_recv()
    project(1 - core, regrouped[:, (groups - 1) * band :], groups - 1)
    updated = (residual[...].astype(f32) + proj[...]).astype(bf16)
    updated = updated.astype(f32)
    proj[...] = updated
    normed[...] = (
        updated
        * lax.rsqrt(jnp.mean(updated * updated, axis=1, keepdims=True) + epsilon)
        * ffn_gain[...]
    ).astype(bf16)

    chunks = vr_sem.shape[1]
    wide = total // chunks

    def part_of(k):
        return pl.ds(k * wide, wide)

    def dense_copy(kind, k, relay):
        return pltpu.make_async_remote_copy(
            src_ref=normed.at[:, part_of(k)], dst_ref=dense_in.at[kind, :, part_of(k)],
            send_sem=vs_sem, recv_sem=vr_sem.at[kind, k],
            device_id={"sp": relay * plane + spot}, device_id_type=MESH,
        )

    def block(r):
        return pl.ds(r * cap, cap)

    def local_rows(device):
        return rows_of(device - first_near, cap)

    def send_copy(r):
        return pltpu.make_async_remote_copy(
            src_ref=outbox.at[local_rows(partner(me, r))], dst_ref=arrived.at[block(r)],
            send_sem=xs_sem, recv_sem=xr_sem.at[r // plane],
            device_id={"sp": partner(me, r)}, device_id_type=MESH,
        )

    def forward_copy(kind, k):
        return pltpu.make_async_remote_copy(
            src_ref=dense_in.at[kind, :, part_of(k)], dst_ref=dense_in.at[kind, :, part_of(k)],
            send_sem=ws_sem, recv_sem=vr_sem.at[kind, k],
            device_id={"sp": partner(me, plane)}, device_id_type=MESH,
        )

    def scatter_copy(kind, r, k):
        return pltpu.make_async_remote_copy(
            src_ref=far_out.at[kind, rows_of(partner(spot, r), cap), part_of(k)],
            dst_ref=arrived.at[block(near + kind * plane + r), part_of(k)],
            send_sem=fs_sem, recv_sem=fr_sem.at[kind, k],
            device_id={"sp": partner(me, r)}, device_id_type=MESH,
        )

    def answer_copy(r, k):
        return pltpu.make_async_remote_copy(
            src_ref=result.at[block(r), part_of(k)],
            dst_ref=returned.at[local_rows(me), part_of(k)],
            send_sem=ys_sem, recv_sem=yr_sem.at[k],
            device_id={"sp": partner(me, r)}, device_id_type=MESH,
        )

    def gather_copy(kind, r, k):
        return pltpu.make_async_remote_copy(
            src_ref=result.at[block(near + kind * plane + r), part_of(k)],
            dst_ref=part_in.at[kind, rows_of(spot, cap), part_of(k)],
            send_sem=gs_sem, recv_sem=gr_sem.at[kind, k],
            device_id={"sp": partner(me, r)}, device_id_type=MESH,
        )

    def inward_copy(kind, k):
        return pltpu.make_async_remote_copy(
            src_ref=dense_out.at[kind, :, part_of(k)], dst_ref=part_add.at[kind, :, part_of(k)],
            send_sem=as_sem, recv_sem=ar_sem.at[kind, k],
            device_id={"sp": partner(me, plane)}, device_id_type=MESH,
        )

    def home_copy(kind, k):
        return pltpu.make_async_remote_copy(
            src_ref=dense_out.at[kind, :, part_of(k)], dst_ref=dense_ret.at[:, part_of(k)],
            send_sem=es_sem, recv_sem=er_sem.at[k],
            device_id={"sp": (far_mid, far_end)[kind] * plane + spot}, device_id_type=MESH,
        )

    not_mid = jnp.logical_not(is_mid)

    @pl.when(not_mid)
    def _():
        for k in range(chunks):
            dense_copy(1, k, far_mid).start()

    @pl.when(is_mid)
    def _():
        for k in range(chunks // 2):
            dense_copy(0, k, far_mid).start()

    outbox[...] = dot(pick[...], normed[...]).astype(bf16)
    for r in range(plane - 1, 0, -1):
        send_copy(r).start()

    for r in range(near - 1, plane - 1, -1):
        send_copy(r).start()

    arrived[block(0), :] = outbox[local_rows(me), :]

    def scatter(kind, k):
        dense_copy(kind, k, far_mid).wait_recv()
        far_out[kind, :, part_of(k)] = dot(
            pick_far[kind], dense_in[kind, :, part_of(k)]
        ).astype(bf16)
        for r in range(plane - 1, 0, -1):
            scatter_copy(kind, r, k).start()
        arrived[block(near + kind * plane), part_of(k)] = far_out[
            kind, rows_of(spot, cap), part_of(k)
        ]

    def relay(kind, k):
        dense_copy(kind, k, far_mid).wait_recv()
        forward_copy(kind, k).start()
        far_out[kind, :, part_of(k)] = dot(
            pick_far[kind], dense_in[kind, :, part_of(k)]
        ).astype(bf16)
        for r in range(plane - 1, 0, -1):
            scatter_copy(kind, r, k).start()
        arrived[block(near + kind * plane), part_of(k)] = far_out[
            kind, rows_of(spot, cap), part_of(k)
        ]

    inner = wg.shape[2]
    rows_each = plane * cap

    def rows_in(group):
        return slice(group * rows_each, (group + 1) * rows_each)

    def raise_up(group, k):
        part = rows_in(group)
        x = arrived[part, part_of(k)]
        for s in range(2):
            g = dot(x, wg[s, part_of(k), :])
            u = dot(x, wu[s, part_of(k), :])
            if k:
                g = g + acc[0, s]
                u = u + acc[1, s]
            if k < chunks - 1:
                acc[0, s] = g
                acc[1, s] = u
            else:
                hidden[s, part, :] = (g / (1.0 + jnp.exp(-g)) * u).astype(bf16)

    def bring_down(group, k):
        part = rows_in(group)
        result[part, part_of(k)] = (
            dot(hidden[0, part, :], wd[0, :, part_of(k)])
            + dot(hidden[1, part, :], wd[1, :, part_of(k)])
        ).astype(bf16)

    def near_arrive(group):
        if group == 0:
            arrivals(arrived.at[pl.ds(cap, (plane - 1) * cap)], xr_sem.at[0])
        else:
            arrivals(arrived.at[pl.ds(plane * cap, plane * cap)], xr_sem.at[1])

    def near_answer(group, parity):
        for k in range(chunks):
            for r in range(group * plane + parity, (group + 1) * plane, 2):
                if r:
                    answer_copy(r, k).start()
        if group + parity == 0:
            returned[local_rows(me), :] = result[block(0), :]

    def far_arrive(kind, k):
        arrivals(
            arrived.at[pl.ds((near + kind * plane + 1) * cap, (plane - 1) * cap), part_of(k)],
            fr_sem.at[kind, k],
        )
        raise_up(2 + kind, k)

    def far_answer(kind, k):
        bring_down(2 + kind, k)
        for r in range(plane - 1, 0, -1):
            gather_copy(kind, r, k).start()
        part_in[kind, rows_of(spot, cap), part_of(k)] = result[
            block(near + kind * plane), part_of(k)
        ]

    def far_partial(kind, k):
        arrivals(
            part_in.at[kind, pl.ds(0, (plane - 1) * cap), part_of(k)], gr_sem.at[kind, k]
        )
        return combined(comb_far[kind], part_in[kind, :, part_of(k)])

    def inward(kind, k):
        dense_out[kind, :, part_of(k)] = far_partial(kind, k).astype(bf16)
        inward_copy(kind, k).start()

    def homeward(kind, k):
        mine = far_partial(kind, k)
        inward_copy(kind, k).wait_recv()
        dense_out[kind, :, part_of(k)] = (
            mine + part_add[kind, :, part_of(k)].astype(f32)
        ).astype(bf16)
        home_copy(kind, k).start()

    def mid_schedule():
        relay(1, 0)
        relay(1, 1)
        for k in range(chunks // 2, chunks):
            dense_copy(0, k, far_mid).start()
        weights_arrive()
        near_arrive(0)
        raise_up(0, 0)
        raise_up(0, 1)
        relay(1, 2)
        raise_up(0, 2)
        raise_up(0, 3)
        relay(1, 3)
        bring_down(0, 0)
        bring_down(0, 1)
        relay(0, 0)
        bring_down(0, 2)
        bring_down(0, 3)
        relay(0, 1)
        far_arrive(1, 0)
        far_arrive(1, 1)
        relay(0, 2)
        far_arrive(1, 2)
        far_arrive(1, 3)
        relay(0, 3)
        far_answer(1, 0)
        far_answer(1, 1)
        far_answer(1, 2)
        far_answer(1, 3)
        near_arrive(1)
        raise_up(1, 0)
        raise_up(1, 1)
        raise_up(1, 2)
        raise_up(1, 3)
        far_arrive(0, 0)
        far_arrive(0, 1)
        far_arrive(0, 2)
        far_arrive(0, 3)
        far_answer(0, 0)
        far_answer(0, 1)
        far_answer(0, 2)
        far_answer(0, 3)
        bring_down(1, 0)
        bring_down(1, 1)
        bring_down(1, 2)
        bring_down(1, 3)
        for group in range(2):
            for parity in range(2):
                near_answer(group, parity)
        homeward(1, 0)
        homeward(1, 1)
        homeward(1, 2)
        homeward(1, 3)
        homeward(0, 0)
        homeward(0, 1)
        homeward(0, 2)
        homeward(0, 3)

    def end_schedule():
        weights_arrive()
        near_arrive(0)
        raise_up(0, 0)
        raise_up(0, 1)
        raise_up(0, 2)
        raise_up(0, 3)
        scatter(1, 0)
        bring_down(0, 0)
        bring_down(0, 1)
        scatter(1, 1)
        bring_down(0, 2)
        bring_down(0, 3)
        near_arrive(1)
        scatter(1, 2)
        raise_up(1, 0)
        raise_up(1, 1)
        scatter(1, 3)
        raise_up(1, 2)
        raise_up(1, 3)
        bring_down(1, 0)
        bring_down(1, 1)
        bring_down(1, 2)
        bring_down(1, 3)
        near_answer(0, 0)
        near_answer(1, 0)
        far_arrive(1, 0)
        far_arrive(1, 1)
        scatter(0, 0)
        far_arrive(1, 2)
        far_arrive(1, 3)
        scatter(0, 1)
        far_answer(1, 0)
        far_answer(1, 1)
        scatter(0, 2)
        far_answer(1, 2)
        far_answer(1, 3)
        scatter(0, 3)
        far_arrive(0, 0)
        inward(1, 0)
        far_arrive(0, 1)
        inward(1, 1)
        far_arrive(0, 2)
        inward(1, 2)
        far_arrive(0, 3)
        inward(1, 3)
        far_answer(0, 0)
        far_answer(0, 1)
        far_answer(0, 2)
        far_answer(0, 3)
        near_answer(1, 1)
        near_answer(0, 1)
        inward(0, 0)
        inward(0, 1)
        inward(0, 2)
        inward(0, 3)

    def weights_arrive():
        for copy in peer + local:
            copy.wait()

    @pl.when(is_mid)
    def _():
        mid_schedule()

    @pl.when(not_mid)
    def _():
        end_schedule()

    for k in range(chunks):
        arrivals(returned.at[pl.ds(0, (near - 1) * cap), part_of(k)], yr_sem.at[k])
        home_copy(0, k).wait_recv()
        layer_out[:, part_of(k)] = (
            proj[:, part_of(k)]
            + combined(comb[...], returned[:, part_of(k)])
            + dense_ret[:, part_of(k)].astype(f32)
        ).astype(bf16)

    departures(dec_recv.at[:, pl.ds(1, n - 1)], ds_sem)
    departures(st_recv.at[:, pl.ds(1, n - 1)], s_sem)
    departures(ret_send.at[:, pl.ds(1, n - 1)], bs_sem)
    departures(info_recv, is_sem)
    departures(regrouped, ms_sem)
    departures(normed, vs_sem)
    departures(outbox.at[pl.ds(cap, (near - 1) * cap)], xs_sem)
    departures(result.at[pl.ds(cap, (near - 1) * cap)], ys_sem)
    departures(arrived.at[pl.ds(0, 2 * (plane - 1) * cap)], fs_sem)
    departures(result.at[pl.ds(0, 2 * (plane - 1) * cap)], gs_sem)

    @pl.when(not_mid)
    def _():
        departures(dense_out, as_sem)

    @pl.when(is_mid)
    def _():
        departures(dense_in, ws_sem)
        departures(dense_out, es_sem)


def solution(mesh):
    n = mesh.shape["sp"]
    vmem = pl.BlockSpec(memory_space=pltpu.VMEM)
    hbm = pl.BlockSpec(memory_space=pl.ANY)
    dma = pltpu.SemaphoreType.DMA

    def body(
        query, forget_logit, value, out_gate, lower_bound, head_gain, residual_in, w_out,
        ffn_gain, routing, route_weight, expert_gate, expert_up, expert_down,
    ):
        length, width = query.shape
        heads = width // HEAD_DIM
        half, model = residual_in.shape
        cap = 2 * half * routing.shape[1] // n
        cap = -(-cap // 16) * 16
        plane = n // 4
        near = 2 * plane
        slots, near_slots = n * cap, near * cap
        chunks = 4
        groups = max(
            g for g in (1, 2, 4) if heads % g == 0 and (g == 1 or width // n % (16 * g) == 0)
        )
        piece = width // n // groups
        inner = expert_gate.shape[2]
        top = routing.shape[1]
        return pl.pallas_call(
            functools.partial(layer_kernel, n, cap),
            out_shape=jax.ShapeDtypeStruct((half, model), bf16),
            in_specs=[hbm] * 14,
            out_specs=vmem,
            scratch_shapes=[
                pltpu.VMEM((length, width), bf16),
                pltpu.VMEM((length, width), bf16),
                pltpu.VMEM((length, width), bf16),
                pltpu.VMEM((length, width), bf16),
                pltpu.VMEM((1, width), f32),
                pltpu.VMEM((1, width), f32),
                pltpu.VMEM((half, model), bf16),
                pltpu.VMEM((1, model), f32),
                pltpu.VMEM((top, half), jnp.int32),
                pltpu.VMEM((top, half), f32),
                pltpu.VMEM(w_out.shape, bf16),
                pltpu.VMEM((length, width), bf16),
                pltpu.VMEM((length, width), bf16),
                pltpu.VMEM((length, width), f32),
                pltpu.VMEM((width, HEAD_DIM), bf16),
                pltpu.VMEM((groups, n, piece, HEAD_DIM), bf16),
                pltpu.VMEM((groups, heads // groups, HEAD_DIM), f32),
                pltpu.VMEM((groups, n, heads // groups, HEAD_DIM), f32),
                pltpu.VMEM((groups, n, piece, HEAD_DIM), bf16),
                pltpu.VMEM((width, HEAD_DIM), bf16),
                pltpu.VMEM((2, half, width), bf16),
                pltpu.VMEM((half, width), bf16),
                pltpu.VMEM((half, model), f32),
                pltpu.VMEM((2, model, inner), bf16),
                pltpu.VMEM((2, model, inner), bf16),
                pltpu.VMEM((2, inner, model), bf16),
                pltpu.VMEM((length, width), f32),
                pltpu.VMEM((half, model), bf16),
                pltpu.VMEM((near_slots, half), bf16),
                pltpu.VMEM((2 * half, near_slots), bf16),
                pltpu.VMEM((2, plane * cap, half), bf16),
                pltpu.VMEM((2, 2 * half, plane * cap), bf16),
                pltpu.VMEM((-(-2 * top // 8) * 8, -(-half // 128) * 128), f32),
                pltpu.VMEM((2, -(-2 * top // 8) * 8, -(-half // 128) * 128), f32),
                pltpu.VMEM((near_slots, model), bf16),
                pltpu.VMEM((slots, model), bf16),
                pltpu.VMEM((2, 2, plane * cap, inner), f32),
                pltpu.VMEM((2, slots, inner), bf16),
                pltpu.VMEM((slots, model), bf16),
                pltpu.VMEM((near_slots, model), bf16),
                pltpu.VMEM((2, half, model), bf16),
                pltpu.VMEM((2, plane * cap, model), bf16),
                pltpu.VMEM((2, plane * cap, model), bf16),
                pltpu.VMEM((2, half, model), bf16),
                pltpu.VMEM((2, half, model), bf16),
                pltpu.VMEM((half, model), bf16),
                dma((10,)), dma,
                dma, dma((groups,)), dma, dma((groups,)), dma, dma((groups,)),
                dma, dma((groups,)), dma((3,)), dma((3,)), dma((3,)),
                dma, dma((2,)), dma, dma((2,)), dma, dma((chunks,)),
                dma, dma((2, chunks)), dma, dma, dma((2, chunks)),
                dma, dma((2, chunks)), dma, dma((2, chunks)), dma, dma((chunks,)),
            ],
            compiler_params=pltpu.CompilerParams(
                collective_id=0, has_side_effects=True, vmem_limit_bytes=60 << 20
            ),
        )(
            query, forget_logit, value, out_gate, lower_bound[None], head_gain[None],
            residual_in, ffn_gain[None], routing.T, route_weight.T, w_out,
            expert_gate, expert_up, expert_down,
        )

    placed = (
        P("sp", "tp"), P("sp", "tp"), P("sp", "tp"), P("sp", "tp"), P("tp"), P("tp"),
        P(("sp", "tp"), None), P(), P(), P(("sp", "tp"), None), P(("sp", "tp"), None),
        P("sp", None, "tp"), P("sp", None, "tp"), P("sp", "tp", None),
    )
    return jax.shard_map(
        body, mesh=mesh, in_specs=placed, out_specs=P(("sp", "tp"), None), check_vma=False
    )
```

```python
import functools

import jax
import jax.numpy as jnp
from jax import lax
from jax.experimental import pallas as pl
from jax.experimental.pallas import tpu as pltpu
from jax.sharding import PartitionSpec as P

HEAD_DIM = 128
MESH = pl.DeviceIdType.MESH
epsilon = 1e-06
f32 = jnp.float32
bf16 = jnp.bfloat16
NT = (((1,), (1,)), ((), ()))
TN = (((0,), (0,)), ((), ()))


def dot(a, b, dims=(((1,), (0,)), ((), ())), precision=None):
    return lax.dot_general(a, b, dims, precision=precision, preferred_element_type=f32)


def rows_of(index, count):
    return pl.ds(pl.multiple_of(index * count, count), count)


def greet(n):
    me, core = lax.axis_index("sp"), lax.axis_index("tp")
    barrier = pltpu.get_barrier_semaphore()
    pl.semaphore_signal(barrier, inc=1, device_id={"tp": 1 - core}, device_id_type=MESH)

    @pl.loop(1, n)
    def _(r):
        pl.semaphore_signal(
            barrier, inc=1, device_id={"sp": lax.rem(me + r, n)}, device_id_type=MESH
        )

    return barrier


def partner(me, r):
    other = me
    step = 1
    while step <= r:
        if r & step:
            other = other + step * (1 - 2 * (me // step % 2))
        step *= 2
    return other


def arrivals(ref, sem):
    peer = {"tp": 1 - lax.axis_index("tp")}
    pltpu.make_async_remote_copy(ref, ref, sem, sem, device_id=peer, device_id_type=MESH).wait_recv()


def departures(ref, sem):
    peer = {"tp": 1 - lax.axis_index("tp")}
    pltpu.make_async_remote_copy(ref, ref, sem, sem, device_id=peer, device_id_type=MESH).wait_send()


def layer_kernel(
    n, cap,
    query_h, logit_h, value_h, gate_h, bound_h, gain_h, residual_h, ffn_gain_h, routing_h,
    weight_h, w_hbm, g_hbm, u_hbm, d_hbm,
    layer_out,
    query, logit, value, gate, bound, gain, residual, ffn_gain, routing, weight,
    w_out, q_scr, k_scr, ho, st_send, st_recv, dec_send, dec_recv, ret_send, ret_recv,
    mixed, regrouped, proj,
    wg, wu, wd, gated, normed, pick, comb, pick_far, comb_far, info_send, info_recv,
    outbox, arrived, acc, hidden, result, returned, dense_in, far_out, part_in, part_add, dense_out, dense_ret,
    in_sem, w_sem, s_sem, r_sem, ds_sem, dr_sem, bs_sem, br_sem, ms_sem, mr_sem,
    l_sem, ps_sem, pr_sem, is_sem, ir_sem, xs_sem, xr_sem, ys_sem, yr_sem,
    vs_sem, vr_sem, ws_sem, fs_sem, fr_sem, gs_sem, gr_sem, as_sem, ar_sem, es_sem, er_sem,
):
    me, core = lax.axis_index("sp"), lax.axis_index("tp")
    length, width = query.shape
    heads = width // HEAD_DIM
    groups, piece = st_recv.shape[0], st_recv.shape[2]
    per = heads // groups
    half = length // 2
    moves = [
        pltpu.make_async_copy(src, dst, in_sem.at[i])
        for i, (src, dst) in enumerate((
            (logit_h, logit), (bound_h, bound), (query_h, query), (value_h, value),
            (routing_h, routing), (weight_h, weight), (gate_h, gate), (gain_h, gain),
            (residual_h, residual), (ffn_gain_h, ffn_gain),
        ))
    ]
    for move in moves:
        move.start()
    barrier = greet(n)
    w_copy = pltpu.make_async_copy(w_hbm, w_out, w_sem)
    homes = ((g_hbm, wg), (u_hbm, wu), (d_hbm, wd))
    local = [
        pltpu.make_async_copy(src.at[0], dst.at[0], l_sem.at[i])
        for i, (src, dst) in enumerate(homes)
    ]
    peer = [
        pltpu.make_async_remote_copy(
            src_ref=src.at[0], dst_ref=dst.at[1],
            send_sem=ps_sem.at[i], recv_sem=pr_sem.at[i],
            device_id={"tp": 1 - core}, device_id_type=MESH,
        )
        for i, (src, dst) in enumerate(homes)
    ]
    w_copy.start()
    for copy in local:
        copy.start()
    for move in moves[:4]:
        move.wait()

    row = lax.broadcasted_iota(jnp.int32, (length, length), 0)
    col = lax.broadcasted_iota(jnp.int32, (length, length), 1)
    causal = row >= col
    tri = causal.astype(f32)
    def owned(g, index):
        return pl.ds(pl.multiple_of(g * per * HEAD_DIM + index * piece, piece), piece)

    def state_copy(g, r):
        return pltpu.make_async_remote_copy(
            src_ref=st_send.at[owned(g, partner(me, r))], dst_ref=st_recv.at[g, r],
            send_sem=s_sem, recv_sem=r_sem.at[g],
            device_id={"sp": partner(me, r)}, device_id_type=MESH,
        )

    def decay_copy(g, r):
        return pltpu.make_async_remote_copy(
            src_ref=dec_send.at[g], dst_ref=dec_recv.at[g, r],
            send_sem=ds_sem, recv_sem=dr_sem.at[g],
            device_id={"sp": partner(me, r)}, device_id_type=MESH,
        )

    def back_copy(g, r):
        return pltpu.make_async_remote_copy(
            src_ref=ret_send.at[g, partner(me, r)], dst_ref=ret_recv.at[owned(g, me)],
            send_sem=bs_sem, recv_sem=br_sem.at[g],
            device_id={"sp": partner(me, r)}, device_id_type=MESH,
        )

    others = range(n - 1, 0, -1)

    def local_state(h):
        c = slice(h * HEAD_DIM, (h + 1) * HEAD_DIM)
        key = (1.0 - bound[:, c]) / (1.0 + jnp.exp(logit[:, c].astype(f32)))
        cum = dot(tri, jnp.log1p(-key), precision=lax.Precision.HIGHEST)
        last = cum[length - 1 :, :]
        mid_cum = 0.5 * last
        q_scr[:, c] = (query[:, c].astype(f32) * jnp.exp(cum - mid_cum)).astype(bf16)
        keys = (key * jnp.exp(mid_cum - cum)).astype(bf16)
        k_scr[:, c] = keys
        st_send[c, :] = (dot(value[:, c], keys, TN) * jnp.exp(mid_cum)).astype(bf16)
        dec_send[h // per, h % per : h % per + 1, :] = last

    def send_states(first, last):
        for g in range(first, last):
            for r in others:
                decay_copy(g, r).start()
                state_copy(g, r).start()

    early = (groups + 1) // 2
    for h in range(early * per):
        local_state(h)
    pl.semaphore_wait(barrier, n)
    send_states(0, early)
    for h in range(early * per, heads):
        local_state(h)
    send_states(early, groups)

    plane = n // 4
    z, spot = me // plane, me % plane
    upper = z // 2
    first_near = 2 * upper * plane
    is_mid = z == 1 + upper
    far_mid, far_end = 2 - upper, 3 - 3 * upper
    my_kind = jnp.where(is_mid, 0, 1)
    near = 2 * plane
    near_slots = near * cap

    for move in moves[4:]:
        move.wait()
    top, count = routing.shape
    owner = lax.broadcasted_iota(jnp.int32, (n, count), 0)
    before = (
        lax.broadcasted_iota(jnp.int32, (count, count), 0)
        < lax.broadcasted_iota(jnp.int32, (count, count), 1)
    ).astype(bf16)
    used = jnp.zeros((n, 1), f32)
    slot_rows, weight_rows = [], []
    for k in range(top):
        hot = (routing[k : k + 1, :] == owner).astype(f32)
        rank = dot(hot.astype(bf16), before) + used
        used = used + jnp.sum(hot, axis=1, keepdims=True)
        slot_rows.append(
            jnp.sum(hot * (rank + owner.astype(f32) * cap), axis=0, keepdims=True)
        )
        weight_rows.append(weight[k : k + 1, :])

    eye = lax.broadcasted_iota(jnp.int32, (count, count), 0) == lax.broadcasted_iota(
        jnp.int32, (count, count), 1
    )

    def column(line):
        return jnp.sum(jnp.where(eye, line, 0.0), axis=1, keepdims=True)

    def tables(chosen_ref, scale_ref, slots, weights):
        lines = chosen_ref.shape[0]
        down = lax.broadcasted_iota(jnp.int32, (lines, count), 0).astype(f32)
        across = lax.broadcasted_iota(jnp.int32, (count, lines), 1).astype(f32)
        chosen = jnp.zeros((lines, count), f32)
        scale = jnp.zeros((count, lines), f32)
        for slot, share in zip(slots, weights):
            chosen = jnp.where(slot == down, 1.0, chosen)
            scale = jnp.where(column(slot) == across, column(share), scale)
        high = scale.astype(bf16)
        chosen_ref[...] = chosen.astype(bf16)
        scale_ref[:count, :] = high
        scale_ref[count:, :] = (scale - high.astype(f32)).astype(bf16)

    def combined(scale, rows):
        both = dot(scale, rows)
        return both[:count] + both[count:]

    def base_of(first):
        return (first * cap).astype(f32)

    tables(pick, comb, [slot - base_of(first_near) for slot in slot_rows], weight_rows)
    info_send[...] = jnp.zeros_like(info_send)
    for k in range(top):
        info_send[k : k + 1, :count] = slot_rows[k]
        info_send[top + k : top + k + 1, :count] = weight_rows[k]

    info_copies = [
        pltpu.make_async_remote_copy(
            src_ref=info_send, dst_ref=info_recv.at[my_kind],
            send_sem=is_sem, recv_sem=ir_sem.at[my_kind],
            device_id={"sp": to * plane + spot}, device_id_type=MESH,
        )
        for i, to in enumerate((far_mid, far_end))
    ]
    for copy in info_copies:
        copy.start()
    for copy in peer:
        copy.start()
    for g in range(groups):
        st_recv[g, 0] = st_send[owned(g, me), :]
        dec_recv[g, 0] = dec_send[g]

    for h in range(heads):
        c = slice(h * HEAD_DIM, (h + 1) * HEAD_DIM)
        scores = jnp.where(causal, dot(q_scr[:, c], k_scr[:, c], NT), 0.0).astype(bf16)
        ho[:, c] = dot(scores, value[:, c])
        g = gate[:, c].astype(f32)
        gated[:, c] = gain[:, c] * (g / (1.0 + jnp.exp(-g)))

    for kind in range(2):
        pltpu.make_async_remote_copy(
            src_ref=info_send, dst_ref=info_recv.at[kind],
            send_sem=is_sem, recv_sem=ir_sem.at[kind],
            device_id={"sp": far_mid * plane + spot}, device_id_type=MESH,
        ).wait_recv()
        tables(
            pick_far.at[kind],
            comb_far.at[kind],
            [info_recv[kind, k : k + 1, :count] - base_of(z * plane) for k in range(top)],
            [info_recv[kind, top + k : top + k + 1, :count] for k in range(top)],
        )

    own_head = me * piece // HEAD_DIM
    for g in range(groups):
        arrivals(dec_recv.at[g, pl.ds(1, n - 1)], dr_sem.at[g])
        arrivals(st_recv.at[g, pl.ds(1, n - 1)], r_sem.at[g])

        def prefix(p, acc):
            r = 0
            step = 1
            while step < n:
                r = r + step * ((me // step + p // step) % 2)
                step *= 2
            last = dec_recv[g, r, pl.ds(own_head, 1), :]
            ret_send[g, p] = (acc * jnp.exp(0.5 * last)).astype(bf16)
            return acc * jnp.exp(last) + st_recv[g, r].astype(f32)

        lax.fori_loop(0, n, prefix, jnp.zeros((piece, HEAD_DIM), f32), unroll=n <= 16)
        for r in others:
            back_copy(g, r).start()
        ret_recv[owned(g, me), :] = ret_send[g, me]

    total = w_out.shape[1]
    tile = 512
    band = per * HEAD_DIM

    def swap_copy(g):
        return pltpu.make_async_remote_copy(
            src_ref=mixed.at[1 - core, :, pl.ds(g * band, band)],
            dst_ref=regrouped.at[:, pl.ds(g * band, band)],
            send_sem=ms_sem, recv_sem=mr_sem.at[g],
            device_id={"tp": 1 - core}, device_id_type=MESH,
        )

    def project(which, source, g, first=False):
        depth = pl.ds(pl.multiple_of(which * width + g * band, band), band)
        for j in range(total // tile):
            cols = slice(j * tile, (j + 1) * tile)
            part = dot(source, w_out[depth, cols])
            proj[:, cols] = part if first else proj[:, cols] + part

    for g in range(groups):
        arrivals(ret_recv.at[pl.ds(g * band, (n - 1) * piece)], br_sem.at[g])
        for h in range(g * per, (g + 1) * per):
            c = slice(h * HEAD_DIM, (h + 1) * HEAD_DIM)
            out = ho[:, c] + dot(q_scr[:, c], ret_recv[c, :], NT)
            out = out * lax.rsqrt(jnp.mean(out * out, axis=1, keepdims=True) + epsilon)
            out = (out * gated[:, c]).astype(bf16)
            mixed[0, :, c] = out[:half]
            mixed[1, :, c] = out[half:]
        swap_copy(g).start()
        if g == 0:
            w_copy.wait()
        project(core, mixed[core, :, g * band : (g + 1) * band], g, first=g == 0)
        if g:
            swap_copy(g - 1).wait_recv()
            project(1 - core, regrouped[:, (g - 1) * band : g * band], g - 1)
    swap_copy(groups - 1).wait_recv()
    project(1 - core, regrouped[:, (groups - 1) * band :], groups - 1)
    updated = (residual[...].astype(f32) + proj[...]).astype(bf16)
    updated = updated.astype(f32)
    proj[...] = updated
    normed[...] = (
        updated
        * lax.rsqrt(jnp.mean(updated * updated, axis=1, keepdims=True) + epsilon)
        * ffn_gain[...]
    ).astype(bf16)

    chunks = vr_sem.shape[1]
    wide = total // chunks

    def part_of(k):
        return pl.ds(k * wide, wide)

    def dense_copy(kind, k, relay):
        return pltpu.make_async_remote_copy(
            src_ref=normed.at[:, part_of(k)], dst_ref=dense_in.at[kind, :, part_of(k)],
            send_sem=vs_sem, recv_sem=vr_sem.at[kind, k],
            device_id={"sp": relay * plane + spot}, device_id_type=MESH,
        )

    def block(r):
        return pl.ds(r * cap, cap)

    def local_rows(device):
        return rows_of(device - first_near, cap)

    def send_copy(r):
        return pltpu.make_async_remote_copy(
            src_ref=outbox.at[local_rows(partner(me, r))], dst_ref=arrived.at[block(r)],
            send_sem=xs_sem, recv_sem=xr_sem.at[r // plane],
            device_id={"sp": partner(me, r)}, device_id_type=MESH,
        )

    def forward_copy(kind, k):
        return pltpu.make_async_remote_copy(
            src_ref=dense_in.at[kind, :, part_of(k)], dst_ref=dense_in.at[kind, :, part_of(k)],
            send_sem=ws_sem, recv_sem=vr_sem.at[kind, k],
            device_id={"sp": partner(me, plane)}, device_id_type=MESH,
        )

    def scatter_copy(kind, r, k):
        return pltpu.make_async_remote_copy(
            src_ref=far_out.at[kind, rows_of(partner(spot, r), cap), part_of(k)],
            dst_ref=arrived.at[block(near + kind * plane + r), part_of(k)],
            send_sem=fs_sem, recv_sem=fr_sem.at[kind, k],
            device_id={"sp": partner(me, r)}, device_id_type=MESH,
        )

    def answer_copy(r, k):
        return pltpu.make_async_remote_copy(
            src_ref=result.at[block(r), part_of(k)],
            dst_ref=returned.at[local_rows(me), part_of(k)],
            send_sem=ys_sem, recv_sem=yr_sem.at[k],
            device_id={"sp": partner(me, r)}, device_id_type=MESH,
        )

    def gather_copy(kind, r, k):
        return pltpu.make_async_remote_copy(
            src_ref=result.at[block(near + kind * plane + r), part_of(k)],
            dst_ref=part_in.at[kind, rows_of(spot, cap), part_of(k)],
            send_sem=gs_sem, recv_sem=gr_sem.at[kind, k],
            device_id={"sp": partner(me, r)}, device_id_type=MESH,
        )

    def inward_copy(kind, k):
        return pltpu.make_async_remote_copy(
            src_ref=dense_out.at[kind, :, part_of(k)], dst_ref=part_add.at[kind, :, part_of(k)],
            send_sem=as_sem, recv_sem=ar_sem.at[kind, k],
            device_id={"sp": partner(me, plane)}, device_id_type=MESH,
        )

    def home_copy(kind, k):
        return pltpu.make_async_remote_copy(
            src_ref=dense_out.at[kind, :, part_of(k)], dst_ref=dense_ret.at[:, part_of(k)],
            send_sem=es_sem, recv_sem=er_sem.at[k],
            device_id={"sp": (far_mid, far_end)[kind] * plane + spot}, device_id_type=MESH,
        )

    not_mid = jnp.logical_not(is_mid)

    @pl.when(not_mid)
    def _():
        for k in range(chunks):
            dense_copy(1, k, far_mid).start()

    @pl.when(is_mid)
    def _():
        for k in range(chunks // 2):
            dense_copy(0, k, far_mid).start()

    outbox[...] = dot(pick[...], normed[...]).astype(bf16)
    for r in range(plane - 1, 0, -1):
        send_copy(r).start()

    for r in range(near - 1, plane - 1, -1):
        send_copy(r).start()

    arrived[block(0), :] = outbox[local_rows(me), :]

    def scatter(kind, k):
        dense_copy(kind, k, far_mid).wait_recv()
        far_out[kind, :, part_of(k)] = dot(
            pick_far[kind], dense_in[kind, :, part_of(k)]
        ).astype(bf16)
        for r in range(plane - 1, 0, -1):
            scatter_copy(kind, r, k).start()
        arrived[block(near + kind * plane), part_of(k)] = far_out[
            kind, rows_of(spot, cap), part_of(k)
        ]

    def relay(kind, k):
        dense_copy(kind, k, far_mid).wait_recv()
        forward_copy(kind, k).start()
        far_out[kind, :, part_of(k)] = dot(
            pick_far[kind], dense_in[kind, :, part_of(k)]
        ).astype(bf16)
        for r in range(plane - 1, 0, -1):
            scatter_copy(kind, r, k).start()
        arrived[block(near + kind * plane), part_of(k)] = far_out[
            kind, rows_of(spot, cap), part_of(k)
        ]

    inner = wg.shape[2]
    rows_each = plane * cap

    def rows_in(group):
        return slice(group * rows_each, (group + 1) * rows_each)

    def raise_up(group, k):
        part = rows_in(group)
        x = arrived[part, part_of(k)]
        for s in range(2):
            g = dot(x, wg[s, part_of(k), :])
            u = dot(x, wu[s, part_of(k), :])
            if k:
                g = g + acc[0, s]
                u = u + acc[1, s]
            if k < chunks - 1:
                acc[0, s] = g
                acc[1, s] = u
            else:
                hidden[s, part, :] = (g / (1.0 + jnp.exp(-g)) * u).astype(bf16)

    def bring_down(group, k):
        part = rows_in(group)
        result[part, part_of(k)] = (
            dot(hidden[0, part, :], wd[0, :, part_of(k)])
            + dot(hidden[1, part, :], wd[1, :, part_of(k)])
        ).astype(bf16)

    def near_arrive(group):
        if group == 0:
            arrivals(arrived.at[pl.ds(cap, (plane - 1) * cap)], xr_sem.at[0])
        else:
            arrivals(arrived.at[pl.ds(plane * cap, plane * cap)], xr_sem.at[1])

    def near_answer(group, parity):
        for k in range(chunks):
            for r in range(group * plane + parity, (group + 1) * plane, 2):
                if r:
                    answer_copy(r, k).start()
        if group + parity == 0:
            returned[local_rows(me), :] = result[block(0), :]

    def far_arrive(kind, k):
        arrivals(
            arrived.at[pl.ds((near + kind * plane + 1) * cap, (plane - 1) * cap), part_of(k)],
            fr_sem.at[kind, k],
        )
        raise_up(2 + kind, k)

    def far_answer(kind, k):
        bring_down(2 + kind, k)
        for r in range(plane - 1, 0, -1):
            gather_copy(kind, r, k).start()
        part_in[kind, rows_of(spot, cap), part_of(k)] = result[
            block(near + kind * plane), part_of(k)
        ]

    def far_partial(kind, k):
        arrivals(
            part_in.at[kind, pl.ds(0, (plane - 1) * cap), part_of(k)], gr_sem.at[kind, k]
        )
        return combined(comb_far[kind], part_in[kind, :, part_of(k)])

    def inward(kind, k):
        dense_out[kind, :, part_of(k)] = far_partial(kind, k).astype(bf16)
        inward_copy(kind, k).start()

    def homeward(kind, k):
        mine = far_partial(kind, k)
        inward_copy(kind, k).wait_recv()
        dense_out[kind, :, part_of(k)] = (
            mine + part_add[kind, :, part_of(k)].astype(f32)
        ).astype(bf16)
        home_copy(kind, k).start()

    def mid_schedule():
        relay(1, 0)
        relay(1, 1)
        for k in range(chunks // 2, chunks):
            dense_copy(0, k, far_mid).start()
        weights_arrive()
        near_arrive(0)
        raise_up(0, 0)
        raise_up(0, 1)
        relay(1, 2)
        raise_up(0, 2)
        raise_up(0, 3)
        relay(1, 3)
        bring_down(0, 0)
        bring_down(0, 1)
        relay(0, 0)
        bring_down(0, 2)
        bring_down(0, 3)
        relay(0, 1)
        far_arrive(1, 0)
        far_arrive(1, 1)
        relay(0, 2)
        far_arrive(1, 2)
        far_arrive(1, 3)
        relay(0, 3)
        far_answer(1, 0)
        far_answer(1, 1)
        far_answer(1, 2)
        far_answer(1, 3)
        near_arrive(1)
        raise_up(1, 0)
        raise_up(1, 1)
        raise_up(1, 2)
        raise_up(1, 3)
        far_arrive(0, 0)
        far_arrive(0, 1)
        far_arrive(0, 2)
        far_arrive(0, 3)
        far_answer(0, 0)
        far_answer(0, 1)
        far_answer(0, 2)
        far_answer(0, 3)
        bring_down(1, 0)
        bring_down(1, 1)
        bring_down(1, 2)
        bring_down(1, 3)
        for group in range(2):
            for parity in range(2):
                near_answer(group, parity)
        homeward(1, 0)
        homeward(1, 1)
        homeward(1, 2)
        homeward(1, 3)
        homeward(0, 0)
        homeward(0, 1)
        homeward(0, 2)
        homeward(0, 3)

    def end_schedule():
        weights_arrive()
        near_arrive(0)
        raise_up(0, 0)
        raise_up(0, 1)
        raise_up(0, 2)
        raise_up(0, 3)
        scatter(1, 0)
        bring_down(0, 0)
        bring_down(0, 1)
        scatter(1, 1)
        bring_down(0, 2)
        bring_down(0, 3)
        near_arrive(1)
        scatter(1, 2)
        raise_up(1, 0)
        raise_up(1, 1)
        scatter(1, 3)
        raise_up(1, 2)
        raise_up(1, 3)
        bring_down(1, 0)
        bring_down(1, 1)
        bring_down(1, 2)
        bring_down(1, 3)
        near_answer(0, 0)
        near_answer(1, 0)
        far_arrive(1, 0)
        far_arrive(1, 1)
        scatter(0, 0)
        far_arrive(1, 2)
        far_arrive(1, 3)
        scatter(0, 1)
        far_answer(1, 0)
        far_answer(1, 1)
        scatter(0, 2)
        far_answer(1, 2)
        far_answer(1, 3)
        scatter(0, 3)
        far_arrive(0, 0)
        inward(1, 0)
        far_arrive(0, 1)
        inward(1, 1)
        far_arrive(0, 2)
        inward(1, 2)
        far_arrive(0, 3)
        inward(1, 3)
        far_answer(0, 0)
        far_answer(0, 1)
        far_answer(0, 2)
        far_answer(0, 3)
        near_answer(1, 1)
        near_answer(0, 1)
        inward(0, 0)
        inward(0, 1)
        inward(0, 2)
        inward(0, 3)

    def weights_arrive():
        for copy in peer + local:
            copy.wait()

    @pl.when(is_mid)
    def _():
        mid_schedule()

    @pl.when(not_mid)
    def _():
        end_schedule()

    for k in range(chunks):
        arrivals(returned.at[pl.ds(0, (near - 1) * cap), part_of(k)], yr_sem.at[k])
        home_copy(0, k).wait_recv()
        layer_out[:, part_of(k)] = (
            proj[:, part_of(k)]
            + combined(comb[...], returned[:, part_of(k)])
            + dense_ret[:, part_of(k)].astype(f32)
        ).astype(bf16)

    departures(dec_recv.at[:, pl.ds(1, n - 1)], ds_sem)
    departures(st_recv.at[:, pl.ds(1, n - 1)], s_sem)
    departures(ret_send.at[:, pl.ds(1, n - 1)], bs_sem)
    departures(info_recv, is_sem)
    departures(regrouped, ms_sem)
    departures(normed, vs_sem)
    departures(outbox.at[pl.ds(cap, (near - 1) * cap)], xs_sem)
    departures(result.at[pl.ds(cap, (near - 1) * cap)], ys_sem)
    departures(arrived.at[pl.ds(0, 2 * (plane - 1) * cap)], fs_sem)
    departures(result.at[pl.ds(0, 2 * (plane - 1) * cap)], gs_sem)

    @pl.when(not_mid)
    def _():
        departures(dense_out, as_sem)

    @pl.when(is_mid)
    def _():
        departures(dense_in, ws_sem)
        departures(dense_out, es_sem)


def solution(mesh):
    n = mesh.shape["sp"]
    vmem = pl.BlockSpec(memory_space=pltpu.VMEM)
    hbm = pl.BlockSpec(memory_space=pl.ANY)
    dma = pltpu.SemaphoreType.DMA

    def body(
        query, forget_logit, value, out_gate, lower_bound, head_gain, residual_in, w_out,
        ffn_gain, routing, route_weight, expert_gate, expert_up, expert_down,
    ):
        length, width = query.shape
        heads = width // HEAD_DIM
        half, model = residual_in.shape
        cap = 2 * half * routing.shape[1] // n
        cap = -(-cap // 16) * 16
        plane = n // 4
        near = 2 * plane
        slots, near_slots = n * cap, near * cap
        chunks = 4
        groups = max(
            g for g in (1, 2, 4) if heads % g == 0 and (g == 1 or width // n % (16 * g) == 0)
        )
        piece = width // n // groups
        inner = expert_gate.shape[2]
        top = routing.shape[1]
        return pl.pallas_call(
            functools.partial(layer_kernel, n, cap),
            out_shape=pltpu.VMEM((half, model), bf16),
            in_specs=[hbm] * 14,
            out_specs=vmem,
            scratch_shapes=[
                pltpu.VMEM((length, width), bf16),
                pltpu.VMEM((length, width), bf16),
                pltpu.VMEM((length, width), bf16),
                pltpu.VMEM((length, width), bf16),
                pltpu.VMEM((1, width), f32),
                pltpu.VMEM((1, width), f32),
                pltpu.VMEM((half, model), bf16),
                pltpu.VMEM((1, model), f32),
                pltpu.VMEM((top, half), jnp.int32),
                pltpu.VMEM((top, half), f32),
                pltpu.VMEM(w_out.shape, bf16),
                pltpu.VMEM((length, width), bf16),
                pltpu.VMEM((length, width), bf16),
                pltpu.VMEM((length, width), f32),
                pltpu.VMEM((width, HEAD_DIM), bf16),
                pltpu.VMEM((groups, n, piece, HEAD_DIM), bf16),
                pltpu.VMEM((groups, heads // groups, HEAD_DIM), f32),
                pltpu.VMEM((groups, n, heads // groups, HEAD_DIM), f32),
                pltpu.VMEM((groups, n, piece, HEAD_DIM), bf16),
                pltpu.VMEM((width, HEAD_DIM), bf16),
                pltpu.VMEM((2, half, width), bf16),
                pltpu.VMEM((half, width), bf16),
                pltpu.VMEM((half, model), f32),
                pltpu.VMEM((2, model, inner), bf16),
                pltpu.VMEM((2, model, inner), bf16),
                pltpu.VMEM((2, inner, model), bf16),
                pltpu.VMEM((length, width), f32),
                pltpu.VMEM((half, model), bf16),
                pltpu.VMEM((near_slots, half), bf16),
                pltpu.VMEM((2 * half, near_slots), bf16),
                pltpu.VMEM((2, plane * cap, half), bf16),
                pltpu.VMEM((2, 2 * half, plane * cap), bf16),
                pltpu.VMEM((-(-2 * top // 8) * 8, -(-half // 128) * 128), f32),
                pltpu.VMEM((2, -(-2 * top // 8) * 8, -(-half // 128) * 128), f32),
                pltpu.VMEM((near_slots, model), bf16),
                pltpu.VMEM((slots, model), bf16),
                pltpu.VMEM((2, 2, plane * cap, inner), f32),
                pltpu.VMEM((2, slots, inner), bf16),
                pltpu.VMEM((slots, model), bf16),
                pltpu.VMEM((near_slots, model), bf16),
                pltpu.VMEM((2, half, model), bf16),
                pltpu.VMEM((2, plane * cap, model), bf16),
                pltpu.VMEM((2, plane * cap, model), bf16),
                pltpu.VMEM((2, half, model), bf16),
                pltpu.VMEM((2, half, model), bf16),
                pltpu.VMEM((half, model), bf16),
                dma((10,)), dma,
                dma, dma((groups,)), dma, dma((groups,)), dma, dma((groups,)),
                dma, dma((groups,)), dma((3,)), dma((3,)), dma((3,)),
                dma, dma((2,)), dma, dma((2,)), dma, dma((chunks,)),
                dma, dma((2, chunks)), dma, dma, dma((2, chunks)),
                dma, dma((2, chunks)), dma, dma((2, chunks)), dma, dma((chunks,)),
            ],
            compiler_params=pltpu.CompilerParams(
                collective_id=0, has_side_effects=True, vmem_limit_bytes=60 << 20
            ),
        )(
            query, forget_logit, value, out_gate, lower_bound[None], head_gain[None],
            residual_in, ffn_gain[None], routing.T, route_weight.T, w_out,
            expert_gate, expert_up, expert_down,
        )

    placed = (
        P("sp", "tp"), P("sp", "tp"), P("sp", "tp"), P("sp", "tp"), P("tp"), P("tp"),
        P(("sp", "tp"), None), P(), P(), P(("sp", "tp"), None), P(("sp", "tp"), None),
        P("sp", None, "tp"), P("sp", None, "tp"), P("sp", "tp", None),
    )
    return jax.shard_map(
        body, mesh=mesh, in_specs=placed, out_specs=P(("sp", "tp"), None), check_vma=False
    )
```
